256 devices in a mesh: fs: 32 (over z, y), tp: 8 (over x, core).
Axes of the slice: x: 4, y: 4, z: 8, core: 2. Of those that a mesh axis runs over, the one named last changes fastest.
Arguments:
- tokens: bfloat16 [8192, 2048], P('fs'), may hold values from -6 to 6
- routes: int32 [8192, 6], P('fs'), may hold values from 0 to 31, all different within a row; in each aligned block of 256 rows (0 to 255, 256 to 511, ...) at most 80 rows name the same one
- route_weights: float32 [8192, 6], P('fs'), may hold values from 0.1 to 1
- norm_gain: float32 [2048], P('fs'), may hold values from 0.1 to 1.9
- expert_gate: float32 [32, 2048, 1024], P(None, 'fs', 'tp'), may hold values from -0.125 to 0.125
- expert_up: float32 [32, 2048, 1024], P(None, 'fs', 'tp'), may hold values from -0.125 to 0.125
- expert_down: float32 [32, 2048, 1024], P(None, 'fs', 'tp'), may hold values from -0.1875 to 0.1875
- shared_gate: float32 [2048, 1024], P('fs', 'tp'), may hold values from -0.125 to 0.125
- shared_up: float32 [2048, 1024], P('fs', 'tp'), may hold values from -0.125 to 0.125
- shared_down: float32 [2048, 1024], P('fs', 'tp'), may hold values from -0.1875 to 0.1875
Outputs:
- layer_output: bfloat16 [8192, 2048], P('fs', 'tp')
- sample_gate: bfloat16 [32, 2048, 1024], P('fs', None, 'tp')
- sample_up: bfloat16 [32, 2048, 1024], P('fs', None, 'tp')
- sample_down: bfloat16 [32, 2048, 1024], P('fs', None, 'tp')
- common_gate: bfloat16 [2048, 1024], P(None, 'tp')
- common_up: bfloat16 [2048, 1024], P(None, 'tp')
- common_down: bfloat16 [2048, 1024], P(None, 'tp')
The draws below stay inside these ranges and needn't reach their ends.
Inputs may be any that keep to these rules, and one draw needn't show every extreme that they name: `routes`: each row names 6 different experts. In each aligned block of 256 rows (the rows of one index of fs) no expert is named by more than 80 rows, a bound that some expert reaches in some blocks.
All inputs are finite; a program needn't handle non-finite values.
Results may differ from the reference program's by a relative error of at most 0.015.
Values may be sent and summed in bfloat16 or wider, within the bound.
No kernel may reach another device: no remote copies, remote signals or barrier semaphores. Data moves between devices by JAX's collectives and lax.ppermute only.
A program may use at most 128 MiB of HBM per device.

```python
import math
import jax
import jax.numpy as jnp
import numpy as np
from jax import lax

D = 2048
FF = 1024
SH = 1024
TOP = 6
TOK_DEV = 256
EXPERTS = 32
CAP = 80
TOKENS = 8192
N_FS = 32
N_TP = 8


def block_scale(stream_key, dims, split, least, high):
    gain = 1.0
    for dim, blocks in split:
        draws = jax.random.uniform(jax.random.fold_in(jax.random.fold_in(stream_key, 6), dim), (blocks,), jnp.float32, least / len(split), high / len(split))
        gain = gain * jnp.repeat(jnp.exp(draws), dims[dim] // blocks).reshape((-1,) + (1,) * (len(dims) - 1 - dim))
    return gain


def deal_out(key, own, number, rows, count, top, bound, slope):
    ranking = jax.random.permutation(key, count)
    heavy_load, ordinary = shares(count, rows * top, bound, slope, True), shares(count, rows * top, bound, slope, False)
    places = jnp.arange(count)

    def named(tallies, rotation):
        used = int((tallies > 0).sum())
        fixed = max(1, used // 4)
        shifted = fixed + (places - fixed + rotation * (used - fixed)) % max(1, count - fixed)
        return jnp.zeros((count,), jnp.int32).at[ranking[jnp.where(places < fixed, places, shifted)]].set(jnp.asarray(tallies, jnp.int32))

    tallies = jnp.where(number % 4 == 0, named(heavy_load, number // 4), named(ordinary, number - number // 4 - 1))
    mixed = jax.random.permutation(jax.random.fold_in(own, 3), count)
    giver, taker = mixed[0:count // 2 * 2:2], mixed[1:count // 2 * 2:2]
    room = jnp.minimum(tallies[giver] - 1, bound - tallies[taker]) // 2
    room = jnp.where((giver == ranking[0]) | (taker == ranking[0]) | (tallies[taker] == 0), 0, jnp.maximum(room, 0))
    shifted = jax.random.randint(jax.random.fold_in(own, 4), (count // 2,), 0, 1 << 20) % (room + 1)
    tallies = tallies.at[giver].add(-shifted).at[taker].add(shifted)
    items = jnp.searchsorted(jnp.cumsum(tallies), jnp.arange(rows * top), side="right").astype(jnp.int32)
    table = items.reshape(top, rows).T
    table = table[jax.random.permutation(jax.random.fold_in(own, 1), rows)]
    rotation = jax.random.randint(jax.random.fold_in(own, 2), (rows, 1), 0, top)
    return jnp.take_along_axis(table, (jnp.arange(top)[None, :] + rotation) % top, axis=1)


def shares(number_of, total, limit, slope, full):
    portions = [(1 << 20) // math.isqrt(grade ** slope) + 1 for grade in range(1, number_of + 1)]
    largest = limit if full else min(limit, max(-(-total // number_of), total * portions[0] // sum(portions)))
    least = 1 if total - largest >= number_of - 1 else 0
    counts, rest = [largest] + [least] * (number_of - 1), total - largest - least * (number_of - 1)
    while rest > 0:
        free = [i for i in range(1, number_of) if counts[i] < largest] or [i for i in range(1, number_of) if counts[i] < limit]
        pool, budget = sum([portions[i] for i in free]), rest
        for i in free:
            extra = min(limit - counts[i], max(1, budget * portions[i] // pool), rest)
            counts[i] = counts[i] + extra
            rest = rest - extra
    return np.array(counts)


def normal_values(stream_key, shape, scale, limit, shards=(), kind=jnp.bfloat16):
    result = scale * jax.random.normal(stream_key, shape, jnp.float32)
    if shards:
        result = result * block_scale(stream_key, shape, shards, -0.22, 0.18)
    return jnp.clip(result, -limit, limit).astype(kind)


def setup_inputs(seed: int = 0) -> dict:
    streams_of = jax.random.split(jax.random.key(seed), 11)
    tokens = normal_values(streams_of[0], (TOKENS, D), 1.0, 6.0, ((0, 32),))
    routes_keys = jax.random.split(jax.random.fold_in(streams_of[1], 1), TOKENS // TOK_DEV)
    routes_turns = jax.random.permutation(jax.random.fold_in(streams_of[1], 3), TOKENS // TOK_DEV)
    routes = jax.vmap(lambda own, number: deal_out(jax.random.fold_in(streams_of[1], 2), own, number, TOK_DEV, EXPERTS, TOP, CAP, 1))(routes_keys, routes_turns).reshape((TOKENS, TOP))
    route_weights = jnp.clip(jnp.exp(math.log(1.0) - 2.3025851 * jax.random.uniform(streams_of[2], (TOKENS, TOP), jnp.float32) ** block_scale(streams_of[2], (TOKENS, TOP), ((0, 32),), -0.2, 0.2)), 0.1, 1.0)
    norm_gain = jnp.clip(1.0 + 0.18 * jax.random.normal(streams_of[3], (D,), jnp.float32), 0.1, 1.9)
    expert_gate = normal_values(streams_of[4], (EXPERTS, D, FF), D ** -0.5, 0.125, ((1, 32), (2, 8)), jnp.float32)
    expert_up = normal_values(streams_of[5], (EXPERTS, D, FF), D ** -0.5, 0.125, ((1, 32), (2, 8)), jnp.float32)
    expert_down = normal_values(streams_of[6], (EXPERTS, D, FF), FF ** -0.5, 0.1875, ((1, 32), (2, 8)), jnp.float32)
    shared_gate = normal_values(streams_of[7], (D, SH), D ** -0.5, 0.125, ((0, 32), (1, 8)), jnp.float32)
    shared_up = normal_values(streams_of[8], (D, SH), D ** -0.5, 0.125, ((0, 32), (1, 8)), jnp.float32)
    shared_down = normal_values(streams_of[9], (D, SH), SH ** -0.5, 0.1875, ((0, 32), (1, 8)), jnp.float32)
    return dict(tokens=tokens, routes=routes, route_weights=route_weights, norm_gain=norm_gain, expert_gate=expert_gate, expert_up=expert_up, expert_down=expert_down, shared_gate=shared_gate, shared_up=shared_up, shared_down=shared_down)


EPSILON = 1e-06

def normalize(tokens):
    values = tokens.astype(jnp.float32)
    scale = lax.rsqrt(lax.optimization_barrier(jnp.mean(values * values, axis=-1, keepdims=True)) + EPSILON)
    return (values * scale).astype(jnp.bfloat16)

def block_sum(hidden, down):
    block_width = hidden.shape[1] // N_TP
    total = jnp.zeros((hidden.shape[0], down.shape[0]), jnp.float32)
    for block in range(N_TP):
        lower = block * block_width
        part = jnp.dot(hidden[:, lower:lower + block_width], down[:, lower:lower + block_width].T, preferred_element_type=jnp.float32).astype(jnp.bfloat16)
        part = lax.optimization_barrier(part)
        total = total + part.astype(jnp.float32)
    return total

def reference(tokens, routes, route_weights, norm_gain, expert_gate, expert_up, expert_down, shared_gate, shared_up, shared_down):
    sample_gate = (norm_gain[None, :, None] * expert_gate).astype(jnp.bfloat16)
    sample_up = (norm_gain[None, :, None] * expert_up).astype(jnp.bfloat16)
    sample_down = expert_down.astype(jnp.bfloat16)
    common_gate = (norm_gain[:, None] * shared_gate).astype(jnp.bfloat16)
    common_up = (norm_gain[:, None] * shared_up).astype(jnp.bfloat16)
    common_down = shared_down.astype(jnp.bfloat16)
    normed = normalize(tokens)
    route_blocks = routes.reshape(N_FS, TOK_DEV * TOP)
    member = (route_blocks[:, :, None] == jnp.arange(EXPERTS, dtype=jnp.int32)[None, None, :]).astype(jnp.int32)
    before = lax.optimization_barrier(jnp.sum((jnp.cumsum(member, axis=1) - member) * member, axis=2))
    block_index = jnp.arange(N_FS, dtype=jnp.int32)[:, None]
    slots = (route_blocks * (N_FS * CAP) + block_index * CAP + before).reshape(-1)
    row_index = (block_index * TOK_DEV + jnp.arange(TOK_DEV * TOP, dtype=jnp.int32)[None, :] // TOP).reshape(-1)
    sources = jnp.full((EXPERTS * N_FS * CAP,), TOKENS, jnp.int32).at[slots].set(row_index)
    padded = jnp.concatenate([normed, jnp.zeros((1, D), jnp.bfloat16)], axis=0)

    def per_expert(operands):
        expert_rows, gate_w, up_w, down_w = operands
        rows = padded[expert_rows]
        gate = jnp.dot(rows, gate_w, preferred_element_type=jnp.float32)
        upward = jnp.dot(rows, up_w, preferred_element_type=jnp.float32)
        hidden = (jax.nn.silu(gate) * upward).astype(jnp.bfloat16)
        return block_sum(hidden, down_w).astype(jnp.bfloat16)
    expert_out = lax.map(per_expert, (sources.reshape(EXPERTS, N_FS * CAP), sample_gate, sample_up, sample_down))
    picked = expert_out.reshape(EXPERTS * N_FS * CAP, D)[slots].astype(jnp.float32).reshape(TOKENS, TOP, D)
    routed = lax.optimization_barrier(jnp.sum(picked * route_weights[:, :, None], axis=1))
    shared_gate_act = jnp.dot(normed, common_gate, preferred_element_type=jnp.float32)
    shared_up_act = jnp.dot(normed, common_up, preferred_element_type=jnp.float32)
    shared_hidden = (jax.nn.silu(shared_gate_act) * shared_up_act).astype(jnp.bfloat16)
    shared_sum = block_sum(shared_hidden, common_down)
    layer_output = (routed + shared_sum).astype(jnp.bfloat16)
    return (layer_output, sample_gate, sample_up, sample_down, common_gate, common_up, common_down)
```

```python
import jax
import jax.numpy as jnp
from jax import lax
from jax.experimental import pallas as pl
from jax.experimental.pallas import tpu as pltpu
from jax.sharding import Mesh
from jax.sharding import PartitionSpec as P

EPSILON = 1e-06
FS = ("z", "y")
TP = ("x", "c")
NZ, NY, NX, NC = 8, 4, 4, 2
EXPERTS = 32
TOK = 256
D = 2048
FF = 1024
SHARE = 10
BF = jnp.bfloat16
F32 = jnp.float32


def iota(shape, dim):
    return lax.broadcasted_iota(jnp.int32, shape, dim)


def dot(a, b):
    return jnp.dot(a, b, preferred_element_type=F32)


def dot_t(a, b):
    return lax.dot_general(a, b, (((1,), (1,)), ((), ())), preferred_element_type=F32)


def flag(condition):
    return jnp.where(condition, 1.0, 0.0).astype(BF)


def shift(array, axis, size, by):
    return lax.ppermute(array, axis, [(i, (i + by) % size) for i in range(size)])


VMEM = pl.BlockSpec(memory_space=pltpu.VMEM)
SMEM = pl.BlockSpec(memory_space=pltpu.SMEM)


def dispatch_kernel(at_ref, tokens_ref, routes_ref, packed_ref, normed_ref):
    base = (at_ref[0] * SHARE).astype(F32)
    values = tokens_ref[...].astype(F32)
    scale = lax.rsqrt(jnp.mean(values * values, axis=-1, keepdims=True) + EPSILON)
    normed = (values * scale).astype(BF)
    normed_ref[...] = normed
    expert = iota((EXPERTS, TOK), 0)
    member = jnp.zeros((EXPERTS, TOK), F32)
    for k in range(routes_ref.shape[0]):
        member = member + jnp.where(routes_ref[k : k + 1, :] == expert, 1.0, 0.0)
    earlier = flag(iota((TOK, TOK), 0) < iota((TOK, TOK), 1))
    position = dot(member.astype(BF), earlier)
    slot = jnp.where(member > 0.0, position, -1.0).astype(BF)
    row = iota((TOK, EXPERTS), 0)
    spread = flag(row // 8 == iota((TOK, EXPERTS), 1))
    slots = dot(spread, slot) - base
    inner = iota((TOK, TOK), 0) % 8
    first = flag(slots == inner.astype(F32))
    packed_ref[:, :D] = dot(first, normed).astype(BF)
    last = slots == (8 + inner % 2).astype(F32)
    tail = jnp.zeros((TOK, 512), F32)
    for j in range(4):
        pick = flag(jnp.logical_and(last, inner // 2 == j))
        tail = tail + dot(pick, normed[:, j * 512 : (j + 1) * 512])
    packed_ref[:, D:] = tail.astype(BF)


def dispatch(tokens, routes_t, at):
    return pl.pallas_call(
        dispatch_kernel,
        out_shape=(
            jax.ShapeDtypeStruct((TOK, D + 512), BF),
            jax.ShapeDtypeStruct((TOK, D), BF),
        ),
        in_specs=[SMEM, VMEM, VMEM],
        out_specs=(VMEM, VMEM),
        compiler_params=pltpu.CompilerParams(vmem_limit_bytes=24 << 20),
        cost_estimate=pl.CostEstimate(flops=10**9, bytes_accessed=4 << 20, transcendentals=0),
        name="dispatch",
    )(at, tokens, routes_t)


def mixing_kernel(core_ref, routes_ref, weights_ref, *out_refs):
    core = core_ref[0]
    expert = iota((TOK, EXPERTS), 1)
    member = jnp.zeros((TOK, EXPERTS), F32)
    weight = jnp.zeros((TOK, EXPERTS), F32)
    for k in range(routes_ref.shape[1]):
        same = routes_ref[:, k : k + 1] == expert
        member = member + jnp.where(same, 1.0, 0.0)
        weight = weight + jnp.where(same, weights_ref[:, k : k + 1], 0.0)
    earlier = flag(iota((TOK, TOK), 1) < iota((TOK, TOK), 0))
    position = dot(earlier, member.astype(BF))
    slot = jnp.where(member > 0.0, position, -1.0).astype(BF)
    high = weight.astype(BF)
    low = (weight - high.astype(F32)).astype(BF)
    lanes = EXPERTS * NX * 8
    spread = flag(iota((EXPERTS, lanes), 1) // (NX * 8) == iota((EXPERTS, lanes), 0))
    slots = dot(slot, spread)
    lane = iota((TOK, lanes), 1)
    start = ((lane // 8) % NX * NC + core) * SHARE
    first = slots == (start + lane % 8).astype(F32)
    last = slots == (start + 8 + lane % 2).astype(F32)
    for part, wide in enumerate((dot(high, spread), dot(low, spread))):
        out_refs[part][...] = jnp.where(first, wide, 0.0).astype(BF)
        out_refs[2 + part][...] = jnp.where(last, wide, 0.0).astype(BF)


def mixing(routes, route_weights, core):
    shape = jax.ShapeDtypeStruct((TOK, EXPERTS * NX * 8), BF)
    return pl.pallas_call(
        mixing_kernel,
        out_shape=(shape,) * 4,
        in_specs=[SMEM, VMEM, VMEM],
        out_specs=(VMEM,) * 4,
        compiler_params=pltpu.CompilerParams(vmem_limit_bytes=24 << 20),
        cost_estimate=pl.CostEstimate(flops=10**9, bytes_accessed=4 << 20, transcendentals=0),
        name="mixing",
    )(core, routes, route_weights)


STEPS = 4


def ffn_kernel(block_ref, gate_ref, up_ref, down_ref, out_ref, rows_ref, total_ref):
    step = pl.program_id(0)

    @pl.when(step == 0)
    def _():
        rows_ref[0:TOK, :] = block_ref[:, :D]
        tail = block_ref[:, D:]
        out_row = iota((64, TOK), 0)
        in_row = iota((64, TOK), 1)
        for j in range(4):
            pick = flag(
                jnp.logical_and(out_row // 2 == in_row // 8, in_row % 8 == 2 * j + out_row % 2)
            )
            rows_ref[TOK : TOK + 64, j * 512 : (j + 1) * 512] = dot(pick, tail).astype(BF)

    rows = rows_ref[...]
    gate = dot(rows, gate_ref[...])
    up = dot(rows, up_ref[...])
    hidden = (gate / (1.0 + jnp.exp(-gate)) * up).astype(BF)
    term = dot_t(hidden, down_ref[...])

    @pl.when(step == 0)
    def _():
        total_ref[...] = term

    @pl.when(step > 0)
    def _():
        total_ref[...] += term

    @pl.when(step == STEPS - 1)
    def _():
        tail = total_ref[TOK : TOK + 64, :].astype(BF)
        out_row = iota((TOK, 64), 0)
        in_row = iota((TOK, 64), 1)
        packed = jnp.zeros((TOK, 512), F32)
        for j in range(4):
            pick = flag(
                jnp.logical_and(in_row // 2 == out_row // 8, out_row % 8 == 2 * j + in_row % 2)
            )
            piece = jnp.concatenate(
                [tail[:, x * 512 + j * 128 : x * 512 + (j + 1) * 128] for x in range(NX)], axis=1
            )
            packed = packed + dot(pick, piece)
        for x in range(NX):
            body = total_ref[0:TOK, x * 512 : (x + 1) * 512]
            out_ref[:, x, :, 0:512] = body.astype(BF).reshape(EXPERTS, 8, 512)
            out_ref[:, x, :, 512:640] = (
                packed[:, x * 128 : (x + 1) * 128].astype(BF).reshape(EXPERTS, 8, 128)
            )


def ffn(block, gate, up, down):
    width = FF // STEPS
    column = pl.BlockSpec((D, width), lambda i: (0, i))
    return pl.pallas_call(
        ffn_kernel,
        out_shape=jax.ShapeDtypeStruct((EXPERTS, NX, 8, 640), BF),
        grid=(STEPS,),
        in_specs=[pl.BlockSpec((TOK, D + 512), lambda i: (0, 0)), column, column, column],
        out_specs=pl.BlockSpec((EXPERTS, NX, 8, 640), lambda i: (0, 0, 0, 0)),
        scratch_shapes=[pltpu.VMEM((TOK + 64, D), BF), pltpu.VMEM((TOK + 64, D), F32)],
        compiler_params=pltpu.CompilerParams(vmem_limit_bytes=40 << 20),
        cost_estimate=pl.CostEstimate(
            flops=6 * 320 * D * FF, bytes_accessed=16 << 20, transcendentals=320 * FF
        ),
        name="ffn",
    )(block, gate, up, down)


def combine_kernel(core_ref, back_ref, fh_ref, fl_ref, lh_ref, ll_ref, own_ref, other_ref):
    core = core_ref[0]
    body = back_ref[:, 0:512]
    tail = back_ref[:, 512:640]
    total = dot(fh_ref[...], body) + dot(fl_ref[...], body)
    lane = iota((TOK, EXPERTS * NX * 8), 1)
    pieces = []
    for j in range(4):
        mine = lane % 8 // 2 == j
        zero = jnp.zeros((), BF)
        pieces.append(
            dot(jnp.where(mine, lh_ref[...], zero), tail)
            + dot(jnp.where(mine, ll_ref[...], zero), tail)
        )
    total = total + jnp.concatenate(pieces, axis=1)
    low, high = total[:, :256], total[:, 256:]
    own_ref[...] = jnp.where(core == 0, low, high)
    other_ref[...] = jnp.where(core == 0, high, low).astype(BF)


def combine(back, mix, core):
    return pl.pallas_call(
        combine_kernel,
        out_shape=(
            jax.ShapeDtypeStruct((TOK, 256), F32),
            jax.ShapeDtypeStruct((TOK, 256), BF),
        ),
        in_specs=[SMEM] + [VMEM] * 5,
        out_specs=(VMEM, VMEM),
        compiler_params=pltpu.CompilerParams(vmem_limit_bytes=24 << 20),
        cost_estimate=pl.CostEstimate(flops=10**9, bytes_accessed=4 << 20, transcendentals=0),
        name="combine",
    )(core, back, *mix)


def place_kernel(at_ref, *refs):
    block_refs, out_refs = refs[:NY], refs[NY:]
    z, y = at_ref[0], at_ref[1]
    for dy in range(NY):
        for dz in range(NZ):
            row = ((z + dz) % NZ * NY + (y + dy) % NY) * 64
            row = pl.multiple_of(row, 64)
            for n in range(3):
                out_refs[n][pl.ds(row, 64), :] = block_refs[dy][dz, :, n * 128 : (n + 1) * 128]


def place(blocks, at):
    shape = jax.ShapeDtypeStruct((D, 128), BF)
    return pl.pallas_call(
        place_kernel,
        out_shape=(shape,) * 3,
        in_specs=[SMEM] + [VMEM] * NY,
        out_specs=(VMEM,) * 3,
        compiler_params=pltpu.CompilerParams(vmem_limit_bytes=16 << 20),
        cost_estimate=pl.CostEstimate(flops=10**8, bytes_accessed=4 << 20, transcendentals=0),
        name="place",
    )(at, *blocks)


def exchange(array, axes):
    return lax.all_to_all(array, axes, split_axis=0, concat_axis=0, tiled=True)


def body(
    tokens,
    routes,
    route_weights,
    norm_gain,
    expert_gate,
    expert_up,
    expert_down,
    shared_gate,
    shared_up,
    shared_down,
):
    z, y, x, c = (lax.axis_index(a).astype(jnp.int32) for a in ("z", "y", "x", "c"))
    at = (x * NC + c).reshape(1)
    core = c.reshape(1)
    gain_rows = norm_gain[None, :, None]

    shared = jnp.concatenate(
        [
            (shared_gate * norm_gain[:, None]).astype(BF),
            (shared_up * norm_gain[:, None]).astype(BF),
            shared_down.astype(BF),
        ],
        axis=1,
    )
    column = jnp.stack([shared] + [shift(shared, "z", NZ, -k) for k in range(1, NZ)])
    blocks = [column] + [shift(column, "y", NY, -k) for k in range(1, NY)]

    gate_rows = exchange((expert_gate * gain_rows).astype(BF), FS).reshape(D, 128)
    up_in, gate_rows = lax.optimization_barrier(
        ((expert_up * gain_rows).astype(BF), gate_rows)
    )
    up_rows = exchange(up_in, FS).reshape(D, 128)
    down_in, up_rows = lax.optimization_barrier((expert_down.astype(BF), up_rows))
    down_rows = exchange(down_in, FS).reshape(D, 128)

    packed, normed = dispatch(tokens, routes.T, at)
    packed, down_rows = lax.optimization_barrier((packed, down_rows))
    whole_gate = lax.all_gather(gate_rows, TP, axis=1, tiled=True)
    whole_up = lax.all_gather(up_rows, TP, axis=1, tiled=True)
    whole_down = lax.all_gather(down_rows, TP, axis=1, tiled=True)
    block = exchange(packed.reshape(EXPERTS, 8, D + 512), FS).reshape(TOK, D + 512)

    common_gate, common_up, common_down = place(blocks, jnp.stack([z, y]))
    shared_hidden = (
        jax.nn.silu(dot(normed, common_gate)) * dot(normed, common_up)
    ).astype(BF)
    shared_terms = dot_t(shared_hidden, common_down).astype(BF)
    shared_terms = jnp.moveaxis(shared_terms.reshape(TOK, NX * NC, 256), 1, 0)
    shared_terms, whole_down = lax.optimization_barrier((shared_terms, whole_down))
    shared_sum = lax.psum_scatter(shared_terms, TP, scatter_dimension=0, tiled=True)[0]

    mix = mixing(routes, route_weights, core)
    results = ffn(block, whole_gate, whole_up, whole_down)
    back = exchange(results.reshape(EXPERTS * NX, 8, 640), ("z", "y", "x"))
    own, other = combine(back.reshape(EXPERTS * NX * 8, 640), mix, core)
    other = shift(other, "c", NC, 1)
    layer_output = (own + other.astype(F32) + shared_sum.astype(F32)).astype(BF)
    return (
        layer_output,
        gate_rows[None],
        up_rows[None],
        down_rows[None],
        common_gate,
        common_up,
        common_down,
    )


def solution(mesh):
    mesh = Mesh(mesh.devices.reshape(NZ, NY, NX, NC), FS + TP)
    return jax.shard_map(
        body,
        mesh=mesh,
        in_specs=(
            P(FS, None),
            P(FS, None),
            P(FS, None),
            P(FS),
            P(None, FS, TP),
            P(None, FS, TP),
            P(None, FS, TP),
            P(FS, TP),
            P(FS, TP),
            P(FS, TP),
        ),
        out_specs=(
            P(FS, TP),
            P(FS, None, TP),
            P(FS, None, TP),
            P(FS, None, TP),
            P(None, TP),
            P(None, TP),
            P(None, TP),
        ),
        check_vma=False,
    )
```

```python
import jax
import jax.numpy as jnp
from jax import lax
from jax.experimental import pallas as pl
from jax.experimental.pallas import tpu as pltpu
from jax.sharding import Mesh
from jax.sharding import PartitionSpec as P

EPSILON = 1e-06
FS = ("z", "y")
TP = ("x", "c")
NZ, NY, NX, NC = 8, 4, 4, 2
EXPERTS = 32
TOK = 256
D = 2048
FF = 1024
SHARE = 10
BF = jnp.bfloat16
F32 = jnp.float32


def iota(shape, dim):
    return lax.broadcasted_iota(jnp.int32, shape, dim)


def dot(a, b):
    return jnp.dot(a, b, preferred_element_type=F32)


def dot_t(a, b):
    return lax.dot_general(a, b, (((1,), (1,)), ((), ())), preferred_element_type=F32)


def flag(condition):
    return jnp.where(condition, 1.0, 0.0).astype(BF)


def shift(array, axis, size, by):
    return lax.ppermute(array, axis, [(i, (i + by) % size) for i in range(size)])


VMEM = pl.BlockSpec(memory_space=pltpu.VMEM)
SMEM = pl.BlockSpec(memory_space=pltpu.SMEM)


def dispatch_kernel(at_ref, tokens_ref, routes_ref, packed_ref, normed_ref):
    base = (at_ref[0] * SHARE).astype(F32)
    values = tokens_ref[...].astype(F32)
    scale = lax.rsqrt(jnp.mean(values * values, axis=-1, keepdims=True) + EPSILON)
    normed = (values * scale).astype(BF)
    normed_ref[...] = normed
    expert = iota((EXPERTS, TOK), 0)
    member = jnp.zeros((EXPERTS, TOK), F32)
    for k in range(routes_ref.shape[0]):
        member = member + jnp.where(routes_ref[k : k + 1, :] == expert, 1.0, 0.0)
    earlier = flag(iota((TOK, TOK), 0) < iota((TOK, TOK), 1))
    position = dot(member.astype(BF), earlier)
    slot = jnp.where(member > 0.0, position, -1.0).astype(BF)
    row = iota((TOK, EXPERTS), 0)
    spread = flag(row // 8 == iota((TOK, EXPERTS), 1))
    slots = dot(spread, slot) - base
    inner = iota((TOK, TOK), 0) % 8
    first = flag(slots == inner.astype(F32))
    packed_ref[:, :D] = dot(first, normed).astype(BF)
    last = slots == (8 + inner % 2).astype(F32)
    tail = jnp.zeros((TOK, 512), F32)
    for j in range(4):
        pick = flag(jnp.logical_and(last, inner // 2 == j))
        tail = tail + dot(pick, normed[:, j * 512 : (j + 1) * 512])
    packed_ref[:, D:] = tail.astype(BF)


def dispatch(tokens, routes_t, at):
    return pl.pallas_call(
        dispatch_kernel,
        out_shape=(
            jax.ShapeDtypeStruct((TOK, D + 512), BF),
            jax.ShapeDtypeStruct((TOK, D), BF),
        ),
        in_specs=[SMEM, VMEM, VMEM],
        out_specs=(VMEM, VMEM),
        compiler_params=pltpu.CompilerParams(vmem_limit_bytes=24 << 20),
        cost_estimate=pl.CostEstimate(flops=10**9, bytes_accessed=4 << 20, transcendentals=0),
        name="dispatch",
    )(at, tokens, routes_t)


def mixing_kernel(core_ref, routes_ref, weights_ref, *out_refs):
    core = core_ref[0]
    expert = iota((TOK, EXPERTS), 1)
    member = jnp.zeros((TOK, EXPERTS), F32)
    weight = jnp.zeros((TOK, EXPERTS), F32)
    for k in range(routes_ref.shape[1]):
        same = routes_ref[:, k : k + 1] == expert
        member = member + jnp.where(same, 1.0, 0.0)
        weight = weight + jnp.where(same, weights_ref[:, k : k + 1], 0.0)
    earlier = flag(iota((TOK, TOK), 1) < iota((TOK, TOK), 0))
    position = dot(earlier, member.astype(BF))
    slot = jnp.where(member > 0.0, position, -1.0).astype(BF)
    high = weight.astype(BF)
    low = (weight - high.astype(F32)).astype(BF)
    lanes = EXPERTS * NX * 8
    spread = flag(iota((EXPERTS, lanes), 1) // (NX * 8) == iota((EXPERTS, lanes), 0))
    slots = dot(slot, spread)
    lane = iota((TOK, lanes), 1)
    start = ((lane // 8) % NX * NC + core) * SHARE
    first = slots == (start + lane % 8).astype(F32)
    last = slots == (start + 8 + lane % 2).astype(F32)
    for part, wide in enumerate((dot(high, spread), dot(low, spread))):
        out_refs[part][...] = jnp.where(first, wide, 0.0).astype(BF)
        out_refs[2 + part][...] = jnp.where(last, wide, 0.0).astype(BF)


def mixing(routes, route_weights, core):
    shape = jax.ShapeDtypeStruct((TOK, EXPERTS * NX * 8), BF)
    return pl.pallas_call(
        mixing_kernel,
        out_shape=(shape,) * 4,
        in_specs=[SMEM, VMEM, VMEM],
        out_specs=(VMEM,) * 4,
        compiler_params=pltpu.CompilerParams(vmem_limit_bytes=24 << 20),
        cost_estimate=pl.CostEstimate(flops=10**9, bytes_accessed=4 << 20, transcendentals=0),
        name="mixing",
    )(core, routes, route_weights)


WAYS = 6
HALF = D // 2


def ffn_kernel(block_ref, *refs):
    source_refs = refs[: 3 * WAYS]
    out_ref, weight_ref, rows_ref, total_ref, hidden_ref, sems = refs[3 * WAYS :]
    copies = []
    for n in range(3):
        own, left, right, near, far, other = source_refs[n * WAYS : (n + 1) * WAYS]
        pieces = [
            (own, weight_ref.at[n, 0]),
            (left, weight_ref.at[n, 1]),
            (right, weight_ref.at[n, 2]),
            (near, weight_ref.at[n, 3, 0:HALF]),
            (far, weight_ref.at[n, 3, HALF:D]),
            (other, weight_ref.at[n, 4:8]),
        ]
        copies.append(
            [
                pltpu.make_async_copy(source, target, sems.at[n, i])
                for i, (source, target) in enumerate(pieces)
            ]
        )
    for group in zip(*copies):
        for copy in group:
            copy.start()

    rows_ref[0:TOK, :] = block_ref[:, :D]
    tail = block_ref[:, D:]
    out_row = iota((64, TOK), 0)
    in_row = iota((64, TOK), 1)
    for j in range(4):
        pick = flag(
            jnp.logical_and(out_row // 2 == in_row // 8, in_row % 8 == 2 * j + out_row % 2)
        )
        rows_ref[TOK : TOK + 64, j * 512 : (j + 1) * 512] = dot(pick, tail).astype(BF)

    def wide(n, first):
        return jnp.concatenate([weight_ref[n, first], weight_ref[n, first + 1]], axis=1)

    def step(first, fresh):
        gate = dot(rows_ref[...], wide(0, first))
        up = dot(rows_ref[...], wide(1, first))
        hidden_ref[...] = (gate / (1.0 + jnp.exp(-gate)) * up).astype(BF)
        for m in range(4):
            part = slice(m * 512, (m + 1) * 512)
            down = jnp.concatenate(
                [weight_ref[2, first, part, :], weight_ref[2, first + 1, part, :]], axis=1
            )
            term = dot_t(hidden_ref[...], down)
            if fresh:
                total_ref[:, part] = term
            else:
                total_ref[:, part] += term

    def wait(first, last):
        for i in range(first, last):
            for n in range(3):
                copies[n][i].wait()

    wait(0, 2)
    step(0, True)
    wait(2, WAYS)

    @pl.loop(1, 4)
    def _(pair):
        step(2 * pair, False)

    tail = total_ref[TOK : TOK + 64, :].astype(BF)
    out_row = iota((TOK, 64), 0)
    in_row = iota((TOK, 64), 1)
    packed = jnp.zeros((TOK, 512), F32)
    for j in range(4):
        pick = flag(
            jnp.logical_and(in_row // 2 == out_row // 8, out_row % 8 == 2 * j + in_row % 2)
        )
        piece = jnp.concatenate(
            [tail[:, x * 512 + j * 128 : x * 512 + (j + 1) * 128] for x in range(NX)], axis=1
        )
        packed = packed + dot(pick, piece)
    for x in range(NX):
        body = total_ref[0:TOK, x * 512 : (x + 1) * 512]
        out_ref[:, x, :, 0:512] = body.astype(BF).reshape(EXPERTS, 8, 512)
        out_ref[:, x, :, 512:640] = (
            packed[:, x * 128 : (x + 1) * 128].astype(BF).reshape(EXPERTS, 8, 128)
        )


def ffn(block, gate, up, down):
    return pl.pallas_call(
        ffn_kernel,
        out_shape=jax.ShapeDtypeStruct((EXPERTS, NX, 8, 640), BF),
        in_specs=[VMEM] + [pl.BlockSpec(memory_space=pl.ANY)] * (3 * WAYS),
        out_specs=VMEM,
        scratch_shapes=[
            pltpu.VMEM((3, 8, D, 128), BF),
            pltpu.VMEM((TOK + 64, D), BF),
            pltpu.VMEM((TOK + 64, D), F32),
            pltpu.VMEM((TOK + 64, 256), BF),
            pltpu.SemaphoreType.DMA((3, WAYS)),
        ],
        compiler_params=pltpu.CompilerParams(vmem_limit_bytes=32 << 20),
        cost_estimate=pl.CostEstimate(
            flops=6 * 320 * D * FF, bytes_accessed=16 << 20, transcendentals=320 * FF
        ),
        name="ffn",
    )(block, *gate, *up, *down)


def combine_kernel(core_ref, back_ref, fh_ref, fl_ref, lh_ref, ll_ref, own_ref, other_ref):
    core = core_ref[0]
    body = back_ref[:, 0:512]
    tail = back_ref[:, 512:640]
    total = dot(fh_ref[...], body) + dot(fl_ref[...], body)
    lane = iota((TOK, EXPERTS * NX * 8), 1)
    pieces = []
    for j in range(4):
        mine = lane % 8 // 2 == j
        zero = jnp.zeros((), BF)
        pieces.append(
            dot(jnp.where(mine, lh_ref[...], zero), tail)
            + dot(jnp.where(mine, ll_ref[...], zero), tail)
        )
    total = total + jnp.concatenate(pieces, axis=1)
    low, high = total[:, :256], total[:, 256:]
    own_ref[...] = jnp.where(core == 0, low, high)
    other_ref[...] = jnp.where(core == 0, high, low).astype(BF)


def combine(back, mix, core):
    return pl.pallas_call(
        combine_kernel,
        out_shape=(
            jax.ShapeDtypeStruct((TOK, 256), F32),
            jax.ShapeDtypeStruct((TOK, 256), BF),
        ),
        in_specs=[SMEM] + [VMEM] * 5,
        out_specs=(VMEM, VMEM),
        compiler_params=pltpu.CompilerParams(vmem_limit_bytes=24 << 20),
        cost_estimate=pl.CostEstimate(flops=10**9, bytes_accessed=4 << 20, transcendentals=0),
        name="combine",
    )(core, back, *mix)


def exchange(array, axes):
    return lax.all_to_all(array, axes, split_axis=0, concat_axis=0, tiled=True)


def after(*arrays):
    return lax.optimization_barrier(arrays)


def to_neighbours(rows):
    return shift(rows, "x", NX, 1), shift(rows, "x", NX, -1)


def to_opposite(near):
    return shift(near[0][:HALF], "x", NX, 1), shift(near[1][HALF:], "x", NX, -1)


def stacked(pieces):
    own, left, right, near, far = pieces
    return [own[None], left[None], right[None], jnp.concatenate([near, far])[None]]


def body(
    tokens,
    routes,
    route_weights,
    norm_gain,
    expert_gate,
    expert_up,
    expert_down,
    shared_gate,
    shared_up,
    shared_down,
):
    x, c = (lax.axis_index(a).astype(jnp.int32) for a in TP)
    at = (x * NC + c).reshape(1)
    core = c.reshape(1)
    gain_rows = norm_gain[None, :, None]

    shared = jnp.concatenate(
        [
            (shared_gate * norm_gain[:, None]).astype(BF),
            (shared_up * norm_gain[:, None]).astype(BF),
            shared_down.astype(BF),
        ],
        axis=1,
    )
    common = lax.all_gather(shared, FS, axis=0, tiled=True)

    gate_in = (expert_gate * gain_rows).astype(BF)
    up_in = (expert_up * gain_rows).astype(BF)
    down_in = expert_down.astype(BF)
    packed, normed = dispatch(tokens, routes.T, at)

    gate_rows = exchange(gate_in, FS).reshape(D, 128)

    up_in, gate_rows = after(up_in, gate_rows)
    up_rows = exchange(up_in, FS).reshape(D, 128)
    gate_near = to_neighbours(gate_rows)

    down_in, up_rows, gate_near = after(down_in, up_rows, gate_near)
    down_rows = exchange(down_in, FS).reshape(D, 128)
    gate_far = to_opposite(gate_near)
    up_near = to_neighbours(up_rows)

    packed, down_rows, gate_far, up_near = after(packed, down_rows, gate_far, up_near)
    block = exchange(packed.reshape(EXPERTS, 8, D + 512), FS).reshape(TOK, D + 512)
    up_far = to_opposite(up_near)
    down_near = to_neighbours(down_rows)
    down_far = to_opposite(down_near)
    gate_all = [gate_rows, *gate_near, *gate_far]
    up_all = [up_rows, *up_near, *up_far]
    down_all = [down_rows, *down_near, *down_far]
    both = shift(jnp.concatenate(stacked(gate_all) + stacked(up_all)), "c", NC, 1)
    gate_all.append(both[:4])
    up_all.append(both[4:])
    down_all.append(shift(jnp.concatenate(stacked(down_all)), "c", NC, 1))

    common_gate, common_up, common_down = jnp.split(common, 3, axis=1)
    shared_hidden = (
        jax.nn.silu(dot(normed, common_gate)) * dot(normed, common_up)
    ).astype(BF)
    shared_terms = dot_t(shared_hidden, common_down).astype(BF)
    shared_terms = jnp.moveaxis(shared_terms.reshape(TOK, NX * NC, 256), 1, 0)
    shared_sum = lax.psum_scatter(shared_terms, TP, scatter_dimension=0, tiled=True)[0]

    mix = mixing(routes, route_weights, core)
    results = ffn(block, gate_all, up_all, down_all)
    back = exchange(results.reshape(EXPERTS * NX, 8, 640), ("z", "y", "x"))
    own, other = combine(back.reshape(EXPERTS * NX * 8, 640), mix, core)
    other = shift(other, "c", NC, 1)
    layer_output = (own + other.astype(F32) + shared_sum.astype(F32)).astype(BF)
    return (
        layer_output,
        gate_rows[None],
        up_rows[None],
        down_rows[None],
        common_gate,
        common_up,
        common_down,
    )


def solution(mesh):
    mesh = Mesh(mesh.devices.reshape(NZ, NY, NX, NC), FS + TP)
    return jax.shard_map(
        body,
        mesh=mesh,
        in_specs=(
            P(FS, None),
            P(FS, None),
            P(FS, None),
            P(FS),
            P(None, FS, TP),
            P(None, FS, TP),
            P(None, FS, TP),
            P(FS, TP),
            P(FS, TP),
            P(FS, TP),
        ),
        out_specs=(
            P(FS, TP),
            P(FS, None, TP),
            P(FS, None, TP),
            P(FS, None, TP),
            P(None, TP),
            P(None, TP),
            P(None, TP),
        ),
        check_vma=False,
    )
```

```python
import jax
import jax.numpy as jnp
from jax import lax
from jax.experimental import pallas as pl
from jax.experimental.pallas import tpu as pltpu
from jax.sharding import Mesh
from jax.sharding import PartitionSpec as P

EPSILON = 1e-06
FS = ("z", "y")
TP = ("x", "c")
NZ, NY, NX, NC = 8, 4, 4, 2
EXPERTS = 32
TOK = 256
D = 2048
FF = 1024
SHARE = 10
BF = jnp.bfloat16
F32 = jnp.float32


def iota(shape, dim):
    return lax.broadcasted_iota(jnp.int32, shape, dim)


def dot(a, b):
    return jnp.dot(a, b, preferred_element_type=F32)


def dot_t(a, b):
    return lax.dot_general(a, b, (((1,), (1,)), ((), ())), preferred_element_type=F32)


def flag(condition):
    return jnp.where(condition, 1.0, 0.0).astype(BF)


def shift(array, axis, size, by):
    return lax.ppermute(array, axis, [(i, (i + by) % size) for i in range(size)])


VMEM = pl.BlockSpec(memory_space=pltpu.VMEM)
SMEM = pl.BlockSpec(memory_space=pltpu.SMEM)
HBM = pl.BlockSpec(memory_space=pltpu.HBM)


def dispatch_kernel(at_ref, tokens_ref, routes_ref, packed_ref, normed_ref):
    base = (at_ref[0] * SHARE).astype(F32)
    values = tokens_ref[...].astype(F32)
    scale = lax.rsqrt(jnp.mean(values * values, axis=-1, keepdims=True) + EPSILON)
    normed = (values * scale).astype(BF)
    normed_ref[...] = normed
    expert = iota((EXPERTS, TOK), 0)
    member = jnp.zeros((EXPERTS, TOK), F32)
    for k in range(routes_ref.shape[0]):
        member = member + jnp.where(routes_ref[k : k + 1, :] == expert, 1.0, 0.0)
    earlier = flag(iota((TOK, TOK), 0) < iota((TOK, TOK), 1))
    position = dot(member.astype(BF), earlier)
    slot = jnp.where(member > 0.0, position, -1.0).astype(BF)
    row = iota((TOK, EXPERTS), 0)
    spread = flag(row // 8 == iota((TOK, EXPERTS), 1))
    slots = dot(spread, slot) - base
    inner = iota((TOK, TOK), 0) % 8
    first = flag(slots == inner.astype(F32))
    packed_ref[:, :D] = dot(first, normed).astype(BF)
    last = slots == (8 + inner % 2).astype(F32)
    tail = jnp.zeros((TOK, 512), F32)
    for j in range(4):
        pick = flag(jnp.logical_and(last, inner // 2 == j))
        tail = tail + dot(pick, normed[:, j * 512 : (j + 1) * 512])
    packed_ref[:, D:] = tail.astype(BF)


def dispatch(tokens, routes_t, at):
    return pl.pallas_call(
        dispatch_kernel,
        out_shape=(
            jax.ShapeDtypeStruct((TOK, D + 512), BF),
            jax.ShapeDtypeStruct((TOK, D), BF),
        ),
        in_specs=[SMEM, VMEM, VMEM],
        out_specs=(VMEM, VMEM),
        compiler_params=pltpu.CompilerParams(vmem_limit_bytes=24 << 20),
        cost_estimate=pl.CostEstimate(flops=10**9, bytes_accessed=4 << 20, transcendentals=0),
        name="dispatch",
    )(at, tokens, routes_t)


WAYS = 6
HALF = D // 2


def ffn_kernel(block_ref, *refs):
    source_refs = refs[: 3 * WAYS]
    out_ref, *sample_refs = refs[3 * WAYS : 3 * WAYS + 4]
    weight_ref, rows_ref, total_ref, hidden_ref, sems, sample_sems = refs[3 * WAYS + 4 :]
    copies = []
    for n in range(3):
        own, left, right, near, far, other = source_refs[n * WAYS : (n + 1) * WAYS]
        pieces = [
            (own, weight_ref.at[n, 0]),
            (left, weight_ref.at[n, 1]),
            (right, weight_ref.at[n, 2]),
            (near, weight_ref.at[n, 3, 0:HALF]),
            (far, weight_ref.at[n, 3, HALF:D]),
            (other, weight_ref.at[n, 4:8]),
        ]
        copies.append(
            [
                pltpu.make_async_copy(source, target, sems.at[n, i])
                for i, (source, target) in enumerate(pieces)
            ]
        )
    for group in zip(*copies):
        for copy in group:
            copy.start()

    rows_ref[0:TOK, :] = block_ref[:, :D]
    tail = block_ref[:, D:]
    out_row = iota((64, TOK), 0)
    in_row = iota((64, TOK), 1)
    for j in range(4):
        pick = flag(
            jnp.logical_and(out_row // 2 == in_row // 8, in_row % 8 == 2 * j + out_row % 2)
        )
        rows_ref[TOK : TOK + 64, j * 512 : (j + 1) * 512] = dot(pick, tail).astype(BF)

    def wide(n, first):
        return jnp.concatenate([weight_ref[n, first], weight_ref[n, first + 1]], axis=1)

    def step(first, fresh):
        gate = dot(rows_ref[...], wide(0, first))
        up = dot(rows_ref[...], wide(1, first))
        hidden_ref[...] = (gate / (1.0 + jnp.exp(-gate)) * up).astype(BF)
        for m in range(4):
            part = slice(m * 512, (m + 1) * 512)
            down = jnp.concatenate(
                [weight_ref[2, first, part, :], weight_ref[2, first + 1, part, :]], axis=1
            )
            term = dot_t(hidden_ref[...], down)
            if fresh:
                total_ref[:, part] = term
            else:
                total_ref[:, part] += term

    def wait(first, last):
        for i in range(first, last):
            for n in range(3):
                copies[n][i].wait()

    wait(0, 2)
    kept = [
        pltpu.make_async_copy(weight_ref.at[n, 0], sample_refs[n].at[0], sample_sems.at[n])
        for n in range(3)
    ]
    for copy in kept:
        copy.start()
    step(0, True)
    wait(2, WAYS)

    @pl.loop(1, 4)
    def _(pair):
        step(2 * pair, False)

    tail = total_ref[TOK : TOK + 64, :].astype(BF)
    out_row = iota((TOK, 64), 0)
    in_row = iota((TOK, 64), 1)
    packed = jnp.zeros((TOK, 512), F32)
    for j in range(4):
        pick = flag(
            jnp.logical_and(in_row // 2 == out_row // 8, out_row % 8 == 2 * j + in_row % 2)
        )
        piece = jnp.concatenate(
            [tail[:, x * 512 + j * 128 : x * 512 + (j + 1) * 128] for x in range(NX)], axis=1
        )
        packed = packed + dot(pick, piece)
    for x in range(NX):
        body = total_ref[0:TOK, x * 512 : (x + 1) * 512]
        out_ref[:, x, :, 0:512] = body.astype(BF).reshape(EXPERTS, 8, 512)
        out_ref[:, x, :, 512:640] = (
            packed[:, x * 128 : (x + 1) * 128].astype(BF).reshape(EXPERTS, 8, 128)
        )
    for copy in kept:
        copy.wait()


def ffn(block, gate, up, down):
    sample = jax.ShapeDtypeStruct((1, D, 128), BF)
    return pl.pallas_call(
        ffn_kernel,
        out_shape=(jax.ShapeDtypeStruct((EXPERTS, NX, 8, 640), BF), sample, sample, sample),
        in_specs=[VMEM] + [HBM] * (3 * WAYS),
        out_specs=(VMEM, HBM, HBM, HBM),
        scratch_shapes=[
            pltpu.VMEM((3, 8, D, 128), BF),
            pltpu.VMEM((TOK + 64, D), BF),
            pltpu.VMEM((TOK + 64, D), F32),
            pltpu.VMEM((TOK + 64, 256), BF),
            pltpu.SemaphoreType.DMA((3, WAYS)),
            pltpu.SemaphoreType.DMA((3,)),
        ],
        compiler_params=pltpu.CompilerParams(vmem_limit_bytes=52 << 20),
        cost_estimate=pl.CostEstimate(
            flops=6 * 320 * D * FF, bytes_accessed=16 << 20, transcendentals=320 * FF
        ),
        name="ffn",
    )(block, *gate, *up, *down)


def combine_kernel(core_ref, routes_ref, weights_ref, back_ref, own_ref, other_ref):
    core = core_ref[0]
    expert = iota((TOK, EXPERTS), 1)
    member = jnp.zeros((TOK, EXPERTS), F32)
    weight = jnp.zeros((TOK, EXPERTS), F32)
    for k in range(routes_ref.shape[1]):
        same = routes_ref[:, k : k + 1] == expert
        member = member + jnp.where(same, 1.0, 0.0)
        weight = weight + jnp.where(same, weights_ref[:, k : k + 1], 0.0)
    earlier = flag(iota((TOK, TOK), 1) < iota((TOK, TOK), 0))
    position = dot(earlier, member.astype(BF))
    slot = jnp.where(member > 0.0, position, -1.0).astype(BF)
    high = weight.astype(BF)
    low = (weight - high.astype(F32)).astype(BF)
    lanes = EXPERTS * NX * 8
    spread = flag(iota((EXPERTS, lanes), 1) // (NX * 8) == iota((EXPERTS, lanes), 0))
    slots = dot(slot, spread)
    lane = iota((TOK, lanes), 1)
    start = ((lane // 8) % NX * NC + core) * SHARE
    first = slots == (start + lane % 8).astype(F32)
    last = slots == (start + 8 + lane % 2).astype(F32)
    body = back_ref[:, 0:512]
    tail = back_ref[:, 512:640]
    total = jnp.zeros((TOK, 512), F32)
    pieces = [jnp.zeros((TOK, 128), F32)] * 4
    for part in (high, low):
        wide = dot(part, spread)
        total = total + dot(jnp.where(first, wide, 0.0).astype(BF), body)
        for j in range(4):
            mine = jnp.logical_and(last, lane % 8 // 2 == j)
            pieces[j] = pieces[j] + dot(jnp.where(mine, wide, 0.0).astype(BF), tail)
    total = total + jnp.concatenate(pieces, axis=1)
    left, right = total[:, :256], total[:, 256:]
    own_ref[...] = jnp.where(core == 0, left, right)
    other_ref[...] = jnp.where(core == 0, right, left).astype(BF)


def combine(back, routes, route_weights, core):
    return pl.pallas_call(
        combine_kernel,
        out_shape=(
            jax.ShapeDtypeStruct((TOK, 256), F32),
            jax.ShapeDtypeStruct((TOK, 256), BF),
        ),
        in_specs=[SMEM] + [VMEM] * 3,
        out_specs=(VMEM, VMEM),
        compiler_params=pltpu.CompilerParams(vmem_limit_bytes=24 << 20),
        cost_estimate=pl.CostEstimate(flops=10**9, bytes_accessed=4 << 20, transcendentals=0),
        name="combine",
    )(core, routes, route_weights, back)


def exchange(array, axes):
    return lax.all_to_all(array, axes, split_axis=0, concat_axis=0, tiled=True)


def after(*arrays):
    return lax.optimization_barrier(arrays)


def to_neighbours(rows):
    return shift(rows, "x", NX, 1), shift(rows, "x", NX, -1)


def to_opposite(near):
    return shift(near[0][:HALF], "x", NX, 1), shift(near[1][HALF:], "x", NX, -1)


def stacked(pieces):
    own, left, right, near, far = pieces
    return [own[None], left[None], right[None], jnp.concatenate([near, far])[None]]


def layer(
    tokens,
    routes,
    route_weights,
    norm_gain,
    expert_gate,
    expert_up,
    expert_down,
    shared_gate,
    shared_up,
    shared_down,
):
    x, c = (lax.axis_index(a).astype(jnp.int32) for a in TP)
    at = (x * NC + c).reshape(1)
    core = c.reshape(1)
    gain_rows = norm_gain[None, :, None]

    shared = jnp.concatenate(
        [
            (shared_gate * norm_gain[:, None]).astype(BF),
            (shared_up * norm_gain[:, None]).astype(BF),
            shared_down.astype(BF),
        ],
        axis=1,
    )
    common = lax.all_gather(shared, FS, axis=0, tiled=True)

    gate_in = (expert_gate * gain_rows).astype(BF)
    gate_in, expert_up, expert_down = after(gate_in, expert_up, expert_down)
    up_in = (expert_up * gain_rows).astype(BF)
    down_in = expert_down.astype(BF)
    packed, normed = dispatch(tokens, routes.T, at)

    gate_rows = exchange(gate_in, FS).reshape(D, 128)

    up_in, gate_rows = after(up_in, gate_rows)
    up_rows = exchange(up_in, FS).reshape(D, 128)
    gate_near = to_neighbours(gate_rows)

    down_in, up_rows, gate_near = after(down_in, up_rows, gate_near)
    down_rows = exchange(down_in, FS).reshape(D, 128)
    gate_far = to_opposite(gate_near)
    up_near = to_neighbours(up_rows)

    packed, down_rows, gate_far, up_near = after(packed, down_rows, gate_far, up_near)
    block = exchange(packed.reshape(EXPERTS, 8, D + 512), FS).reshape(TOK, D + 512)
    up_far = to_opposite(up_near)
    down_near = to_neighbours(down_rows)
    down_far = to_opposite(down_near)
    gate_all = [gate_rows, *gate_near, *gate_far]
    up_all = [up_rows, *up_near, *up_far]
    down_all = [down_rows, *down_near, *down_far]
    both = shift(jnp.concatenate(stacked(gate_all) + stacked(up_all)), "c", NC, 1)
    gate_all.append(both[:4])
    up_all.append(both[4:])
    down_all.append(shift(jnp.concatenate(stacked(down_all)), "c", NC, 1))

    common_gate, common_up, common_down = jnp.split(common, 3, axis=1)
    shared_hidden = (
        jax.nn.silu(dot(normed, common_gate)) * dot(normed, common_up)
    ).astype(BF)
    shared_terms = dot_t(shared_hidden, common_down).astype(BF)
    shared_terms = jnp.moveaxis(shared_terms.reshape(TOK, NX * NC, 256), 1, 0)
    shared_sum = lax.psum_scatter(shared_terms, TP, scatter_dimension=0, tiled=True)[0]

    results, sample_gate, sample_up, sample_down = ffn(block, gate_all, up_all, down_all)
    back = exchange(results.reshape(EXPERTS * NX, 8, 640), ("z", "y", "x"))
    own, other = combine(back.reshape(EXPERTS * NX * 8, 640), routes, route_weights, core)
    other = shift(other, "c", NC, 1)
    layer_output = (own + other.astype(F32) + shared_sum.astype(F32)).astype(BF)
    return (
        layer_output,
        sample_gate,
        sample_up,
        sample_down,
        common_gate,
        common_up,
        common_down,
    )


def solution(mesh):
    mesh = Mesh(mesh.devices.reshape(NZ, NY, NX, NC), FS + TP)
    return jax.shard_map(
        layer,
        mesh=mesh,
        in_specs=(
            P(FS, None),
            P(FS, None),
            P(FS, None),
            P(FS),
            P(None, FS, TP),
            P(None, FS, TP),
            P(None, FS, TP),
            P(FS, TP),
            P(FS, TP),
            P(FS, TP),
        ),
        out_specs=(
            P(FS, TP),
            P(FS, None, TP),
            P(FS, None, TP),
            P(FS, None, TP),
            P(None, TP),
            P(None, TP),
            P(None, TP),
        ),
        check_vma=False,
    )
```

```python
import jax
import jax.numpy as jnp
from jax import lax
from jax.experimental import pallas as pl
from jax.experimental.pallas import tpu as pltpu
from jax.sharding import Mesh
from jax.sharding import PartitionSpec as P

EPSILON = 1e-06
FS = ("z", "y")
TP = ("x", "c")
NZ, NY, NX, NC = 8, 4, 4, 2
EXPERTS = 32
TOK = 256
D = 2048
FF = 1024
SHARE = 10
BF = jnp.bfloat16
F32 = jnp.float32


def iota(shape, dim):
    return lax.broadcasted_iota(jnp.int32, shape, dim)


def dot(a, b):
    return jnp.dot(a, b, preferred_element_type=F32)


def dot_t(a, b):
    return lax.dot_general(a, b, (((1,), (1,)), ((), ())), preferred_element_type=F32)


def flag(condition):
    return jnp.where(condition, 1.0, 0.0).astype(BF)


def shift(array, axis, size, by):
    return lax.ppermute(array, axis, [(i, (i + by) % size) for i in range(size)])


VMEM = pl.BlockSpec(memory_space=pltpu.VMEM)
SMEM = pl.BlockSpec(memory_space=pltpu.SMEM)
HBM = pl.BlockSpec(memory_space=pltpu.HBM)


def dispatch_kernel(at_ref, tokens_ref, routes_ref, packed_ref, normed_ref):
    base = (at_ref[0] * SHARE).astype(F32)
    values = tokens_ref[...].astype(F32)
    scale = lax.rsqrt(jnp.mean(values * values, axis=-1, keepdims=True) + EPSILON)
    normed = (values * scale).astype(BF)
    normed_ref[...] = normed
    expert = iota((EXPERTS, TOK), 0)
    member = jnp.zeros((EXPERTS, TOK), F32)
    for k in range(routes_ref.shape[0]):
        member = member + jnp.where(routes_ref[k : k + 1, :] == expert, 1.0, 0.0)
    earlier = flag(iota((TOK, TOK), 0) < iota((TOK, TOK), 1))
    position = dot(member.astype(BF), earlier)
    slot = jnp.where(member > 0.0, position, -1.0).astype(BF)
    row = iota((TOK, EXPERTS), 0)
    spread = flag(row // 8 == iota((TOK, EXPERTS), 1))
    slots = dot(spread, slot) - base
    inner = iota((TOK, TOK), 0) % 8
    first = flag(slots == inner.astype(F32))
    packed_ref[:, :D] = dot(first, normed).astype(BF)
    last = slots == (8 + inner % 2).astype(F32)
    tail = jnp.zeros((TOK, 512), F32)
    for j in range(4):
        pick = flag(jnp.logical_and(last, inner // 2 == j))
        tail = tail + dot(pick, normed[:, j * 512 : (j + 1) * 512])
    packed_ref[:, D:] = tail.astype(BF)


def dispatch(tokens, routes_t, at):
    return pl.pallas_call(
        dispatch_kernel,
        out_shape=(
            jax.ShapeDtypeStruct((TOK, D + 512), BF),
            jax.ShapeDtypeStruct((TOK, D), BF),
        ),
        in_specs=[SMEM, VMEM, VMEM],
        out_specs=(VMEM, VMEM),
        compiler_params=pltpu.CompilerParams(vmem_limit_bytes=24 << 20),
        cost_estimate=pl.CostEstimate(flops=10**9, bytes_accessed=4 << 20, transcendentals=0),
        name="dispatch",
    )(at, tokens, routes_t)


def round_kernel(gain_ref, gate_ref, up_ref, out_ref):
    gain = gain_ref[...]
    out_ref[:, 0] = (gate_ref[...] * gain[None]).astype(BF)
    out_ref[:, 1] = (up_ref[...] * gain[None]).astype(BF)


def round_both(gain, gate, up):
    block = pl.BlockSpec((8, 64, 128), lambda i: (i, 0, 0))
    return pl.pallas_call(
        round_kernel,
        out_shape=jax.ShapeDtypeStruct((EXPERTS, 2, 64, 128), BF),
        grid=(EXPERTS // 8,),
        in_specs=[pl.BlockSpec((64, 1), lambda i: (0, 0)), block, block],
        out_specs=pl.BlockSpec((8, 2, 64, 128), lambda i: (i, 0, 0, 0)),
        compiler_params=pltpu.CompilerParams(vmem_limit_bytes=16 << 20),
        cost_estimate=pl.CostEstimate(flops=10**7, bytes_accessed=3 << 20, transcendentals=0),
        name="round_both",
    )(gain.reshape(64, 1), gate, up)


WAYS = 10
HALF = 16


def ffn_kernel(block_ref, *refs):
    both_refs, single_refs = refs[:WAYS], refs[WAYS : 2 * WAYS]
    out_ref, *sample_refs = refs[2 * WAYS : 2 * WAYS + 4]
    weight_ref, rows_ref, total_ref, hidden_ref, sems, sample_sems = refs[2 * WAYS + 4 :]
    places = []
    for side in range(2):
        at = 4 * side
        places += [(at, slice(None)), (at + 1, slice(None)), (at + 2, slice(None))]
        places += [(at + 3, slice(0, HALF)), (at + 3, slice(HALF, None))]
    copies = {}
    for i, (at, part) in enumerate(places):
        for n in range(3):
            source = both_refs[i].at[:, n] if n < 2 else single_refs[i]
            target = weight_ref.at[n, at, part]
            copies[n, i] = pltpu.make_async_copy(source, target, sems.at[n, i])
            copies[n, i].start()

    rows_ref[0:TOK, :] = block_ref[:, :D]
    tail = block_ref[:, D:]
    out_row = iota((64, TOK), 0)
    in_row = iota((64, TOK), 1)
    for j in range(4):
        pick = flag(
            jnp.logical_and(out_row // 2 == in_row // 8, in_row % 8 == 2 * j + out_row % 2)
        )
        rows_ref[TOK : TOK + 64, j * 512 : (j + 1) * 512] = dot(pick, tail).astype(BF)

    def wide(n, pair, part=slice(None)):
        return jnp.concatenate(
            [weight_ref[n, 2 * pair + i, part].reshape(-1, 128) for i in range(2)], axis=1
        )

    kept = []
    for pair in range(4):
        needed = [i for i, (at, _) in enumerate(places) if at // 2 == pair]
        for n in range(2):
            for i in needed:
                copies[n, i].wait()
        gate = dot(rows_ref[...], wide(0, pair))
        up = dot(rows_ref[...], wide(1, pair))
        hidden_ref[...] = (gate / (1.0 + jnp.exp(-gate)) * up).astype(BF)
        for i in needed:
            copies[2, i].wait()
        for m in range(4):
            term = dot_t(hidden_ref[...], wide(2, pair, slice(m * 8, (m + 1) * 8)))
            if pair == 0:
                total_ref[:, m * 512 : (m + 1) * 512] = term
            else:
                total_ref[:, m * 512 : (m + 1) * 512] += term
        if pair == 0:
            for n in range(3):
                kept.append(
                    pltpu.make_async_copy(
                        weight_ref.at[n, 0], sample_refs[n], sample_sems.at[n]
                    )
                )
                kept[n].start()

    tail = total_ref[TOK : TOK + 64, :].astype(BF)
    out_row = iota((TOK, 64), 0)
    in_row = iota((TOK, 64), 1)
    packed = jnp.zeros((TOK, 512), F32)
    for j in range(4):
        pick = flag(
            jnp.logical_and(in_row // 2 == out_row // 8, out_row % 8 == 2 * j + in_row % 2)
        )
        piece = jnp.concatenate(
            [tail[:, x * 512 + j * 128 : x * 512 + (j + 1) * 128] for x in range(NX)], axis=1
        )
        packed = packed + dot(pick, piece)
    for x in range(NX):
        body = total_ref[0:TOK, x * 512 : (x + 1) * 512]
        out_ref[:, x, :, 0:512] = body.astype(BF).reshape(EXPERTS, 8, 512)
        out_ref[:, x, :, 512:640] = (
            packed[:, x * 128 : (x + 1) * 128].astype(BF).reshape(EXPERTS, 8, 128)
        )
    for copy in kept:
        copy.wait()


def ffn(block, both, single):
    sample = jax.ShapeDtypeStruct((EXPERTS, 64, 128), BF)
    return pl.pallas_call(
        ffn_kernel,
        out_shape=(jax.ShapeDtypeStruct((EXPERTS, NX, 8, 640), BF), sample, sample, sample),
        in_specs=[VMEM] + [HBM] * (2 * WAYS),
        out_specs=(VMEM, HBM, HBM, HBM),
        scratch_shapes=[
            pltpu.VMEM((3, 8, EXPERTS, 64, 128), BF),
            pltpu.VMEM((TOK + 64, D), BF),
            pltpu.VMEM((TOK + 64, D), F32),
            pltpu.VMEM((TOK + 64, 256), BF),
            pltpu.SemaphoreType.DMA((3, WAYS)),
            pltpu.SemaphoreType.DMA((3,)),
        ],
        compiler_params=pltpu.CompilerParams(vmem_limit_bytes=52 << 20),
        cost_estimate=pl.CostEstimate(
            flops=6 * 320 * D * FF, bytes_accessed=16 << 20, transcendentals=320 * FF
        ),
        name="ffn",
    )(block, *both, *single)


def combine_kernel(core_ref, routes_ref, weights_ref, back_ref, own_ref, other_ref):
    core = core_ref[0]
    expert = iota((TOK, EXPERTS), 1)
    member = jnp.zeros((TOK, EXPERTS), F32)
    weight = jnp.zeros((TOK, EXPERTS), F32)
    for k in range(routes_ref.shape[1]):
        same = routes_ref[:, k : k + 1] == expert
        member = member + jnp.where(same, 1.0, 0.0)
        weight = weight + jnp.where(same, weights_ref[:, k : k + 1], 0.0)
    earlier = flag(iota((TOK, TOK), 1) < iota((TOK, TOK), 0))
    position = dot(earlier, member.astype(BF))
    slot = jnp.where(member > 0.0, position, -1.0).astype(BF)
    high = weight.astype(BF)
    low = (weight - high.astype(F32)).astype(BF)
    lanes = EXPERTS * NX * 8
    spread = flag(iota((EXPERTS, lanes), 1) // (NX * 8) == iota((EXPERTS, lanes), 0))
    slots = dot(slot, spread)
    lane = iota((TOK, lanes), 1)
    start = ((lane // 8) % NX * NC + core) * SHARE
    first = slots == (start + lane % 8).astype(F32)
    last = slots == (start + 8 + lane % 2).astype(F32)
    body = back_ref[:, 0:512]
    tail = back_ref[:, 512:640]
    total = jnp.zeros((TOK, 512), F32)
    pieces = [jnp.zeros((TOK, 128), F32)] * 4
    for part in (high, low):
        wide = dot(part, spread)
        total = total + dot(jnp.where(first, wide, 0.0).astype(BF), body)
        for j in range(4):
            mine = jnp.logical_and(last, lane % 8 // 2 == j)
            pieces[j] = pieces[j] + dot(jnp.where(mine, wide, 0.0).astype(BF), tail)
    total = total + jnp.concatenate(pieces, axis=1)
    left, right = total[:, :256], total[:, 256:]
    own_ref[...] = jnp.where(core == 0, left, right)
    other_ref[...] = jnp.where(core == 0, right, left).astype(BF)


def combine(back, routes, route_weights, core):
    return pl.pallas_call(
        combine_kernel,
        out_shape=(
            jax.ShapeDtypeStruct((TOK, 256), F32),
            jax.ShapeDtypeStruct((TOK, 256), BF),
        ),
        in_specs=[SMEM] + [VMEM] * 3,
        out_specs=(VMEM, VMEM),
        compiler_params=pltpu.CompilerParams(vmem_limit_bytes=24 << 20),
        cost_estimate=pl.CostEstimate(flops=10**9, bytes_accessed=4 << 20, transcendentals=0),
        name="combine",
    )(core, routes, route_weights, back)


def shared_kernel(normed_ref, common_ref, terms_ref, *common_refs):
    for n in range(3):
        common_refs[n][...] = common_ref[:, n * 128 : (n + 1) * 128]
    act = dot(normed_ref[...], common_ref[:, 0:256])
    gate, up = act[:, 0:128], act[:, 128:256]
    hidden = (gate / (1.0 + jnp.exp(-gate)) * up).astype(BF)
    for n in range(NX * NC):
        terms_ref[n] = dot_t(hidden, common_ref[n * 256 : (n + 1) * 256, 256:384]).astype(BF)


def shared_expert(normed, common):
    shape = jax.ShapeDtypeStruct((D, 128), BF)
    return pl.pallas_call(
        shared_kernel,
        out_shape=(jax.ShapeDtypeStruct((NX * NC, TOK, 256), BF), shape, shape, shape),
        in_specs=[VMEM] * 2,
        out_specs=(VMEM,) * 4,
        compiler_params=pltpu.CompilerParams(vmem_limit_bytes=24 << 20),
        cost_estimate=pl.CostEstimate(
            flops=6 * TOK * D * 128, bytes_accessed=6 << 20, transcendentals=TOK * 128
        ),
        name="shared_expert",
    )(normed, common)


def exchange(array, axes):
    return lax.all_to_all(array, axes, split_axis=0, concat_axis=0, tiled=True)


def after(*arrays):
    return lax.optimization_barrier(arrays)


def to_neighbours(rows):
    return shift(rows, "x", NX, 1), shift(rows, "x", NX, -1)


def to_opposite(near):
    return shift(near[0][:HALF], "x", NX, 1), shift(near[1][HALF:], "x", NX, -1)


def layer(
    tokens,
    routes,
    route_weights,
    norm_gain,
    expert_gate,
    expert_up,
    expert_down,
    shared_gate,
    shared_up,
    shared_down,
):
    x, c = (lax.axis_index(a).astype(jnp.int32) for a in TP)
    at = (x * NC + c).reshape(1)
    core = c.reshape(1)

    shared = jnp.concatenate(
        [
            (shared_gate * norm_gain[:, None]).astype(BF),
            (shared_up * norm_gain[:, None]).astype(BF),
            shared_down.astype(BF),
        ],
        axis=1,
    )
    common = lax.all_gather(shared, FS, axis=0, tiled=True)

    both_in = round_both(norm_gain, expert_gate, expert_up)
    both_in, expert_down = after(both_in, expert_down)
    down_in = expert_down.astype(BF)
    packed, normed = dispatch(tokens, routes.T, at)

    both_rows = exchange(both_in, FS)

    down_in, both_rows = after(down_in, both_rows)
    down_rows = exchange(down_in, FS)
    both_near = to_neighbours(both_rows)

    packed, down_rows = after(packed, down_rows)
    block = exchange(packed.reshape(EXPERTS, 8, D + 512), FS).reshape(TOK, D + 512)
    both_far = to_opposite(both_near)
    down_near = to_neighbours(down_rows)
    down_far = to_opposite(down_near)
    both_all = [both_rows, *both_near, *both_far]
    down_all = [down_rows, *down_near, *down_far]
    both_all += [shift(piece, "c", NC, 1) for piece in both_all]
    down_all += [shift(piece, "c", NC, 1) for piece in down_all]

    shared_terms, common_gate, common_up, common_down = shared_expert(normed, common)
    shared_sum = lax.psum_scatter(shared_terms, TP, scatter_dimension=0, tiled=True)[0]

    results, sample_gate, sample_up, sample_down = ffn(block, both_all, down_all)
    back = exchange(results.reshape(EXPERTS * NX, 8, 640), ("z", "y", "x"))
    own, other = combine(back.reshape(EXPERTS * NX * 8, 640), routes, route_weights, core)
    other = shift(other, "c", NC, 1)
    layer_output = (own + other.astype(F32) + shared_sum.astype(F32)).astype(BF)
    return (
        layer_output,
        sample_gate.reshape(1, D, 128),
        sample_up.reshape(1, D, 128),
        sample_down.reshape(1, D, 128),
        common_gate,
        common_up,
        common_down,
    )


def solution(mesh):
    mesh = Mesh(mesh.devices.reshape(NZ, NY, NX, NC), FS + TP)
    return jax.shard_map(
        layer,
        mesh=mesh,
        in_specs=(
            P(FS, None),
            P(FS, None),
            P(FS, None),
            P(FS),
            P(None, FS, TP),
            P(None, FS, TP),
            P(None, FS, TP),
            P(FS, TP),
            P(FS, TP),
            P(FS, TP),
        ),
        out_specs=(
            P(FS, TP),
            P(FS, None, TP),
            P(FS, None, TP),
            P(FS, None, TP),
            P(None, TP),
            P(None, TP),
            P(None, TP),
        ),
        check_vma=False,
    )
```

```python
import jax
import jax.numpy as jnp
from jax import lax
from jax.experimental import pallas as pl
from jax.experimental.pallas import tpu as pltpu
from jax.sharding import Mesh
from jax.sharding import PartitionSpec as P

EPSILON = 1e-06
FS = ("z", "y")
TP = ("x", "c")
NZ, NY, NX, NC = 8, 4, 4, 2
EXPERTS = 32
TOK = 256
D = 2048
FF = 1024
SHARE = 10
BF = jnp.bfloat16
F32 = jnp.float32


def iota(shape, dim):
    return lax.broadcasted_iota(jnp.int32, shape, dim)


def dot(a, b):
    return jnp.dot(a, b, preferred_element_type=F32)


def dot_t(a, b):
    return lax.dot_general(a, b, (((1,), (1,)), ((), ())), preferred_element_type=F32)


def flag(condition):
    return jnp.where(condition, 1.0, 0.0).astype(BF)


def shift(array, axis, size, by):
    return lax.ppermute(array, axis, [(i, (i + by) % size) for i in range(size)])


VMEM = pl.BlockSpec(memory_space=pltpu.VMEM)
SMEM = pl.BlockSpec(memory_space=pltpu.SMEM)
HBM = pl.BlockSpec(memory_space=pltpu.HBM)


def dispatch_kernel(at_ref, tokens_ref, routes_ref, packed_ref, normed_ref):
    base = (at_ref[0] * SHARE).astype(F32)
    values = tokens_ref[...].astype(F32)
    scale = lax.rsqrt(jnp.mean(values * values, axis=-1, keepdims=True) + EPSILON)
    normed = (values * scale).astype(BF)
    normed_ref[...] = normed
    expert = iota((EXPERTS, TOK), 0)
    member = jnp.zeros((EXPERTS, TOK), F32)
    for k in range(routes_ref.shape[0]):
        member = member + jnp.where(routes_ref[k : k + 1, :] == expert, 1.0, 0.0)
    earlier = flag(iota((TOK, TOK), 0) < iota((TOK, TOK), 1))
    position = dot(member.astype(BF), earlier)
    slot = jnp.where(member > 0.0, position, -1.0).astype(BF)
    row = iota((TOK, EXPERTS), 0)
    spread = flag(row // 8 == iota((TOK, EXPERTS), 1))
    slots = dot(spread, slot) - base
    inner = iota((TOK, TOK), 0) % 8
    first = flag(slots == inner.astype(F32))
    packed_ref[:, :D] = dot(first, normed).astype(BF)
    last = slots == (8 + inner % 2).astype(F32)
    tail = jnp.zeros((TOK, 512), F32)
    for j in range(4):
        pick = flag(jnp.logical_and(last, inner // 2 == j))
        tail = tail + dot(pick, normed[:, j * 512 : (j + 1) * 512])
    packed_ref[:, D:] = tail.astype(BF)


def dispatch(tokens, routes_t, at):
    return pl.pallas_call(
        dispatch_kernel,
        out_shape=(
            jax.ShapeDtypeStruct((TOK, D + 512), BF),
            jax.ShapeDtypeStruct((TOK, D), BF),
        ),
        in_specs=[SMEM, VMEM, VMEM],
        out_specs=(VMEM, VMEM),
        compiler_params=pltpu.CompilerParams(vmem_limit_bytes=24 << 20),
        cost_estimate=pl.CostEstimate(flops=10**9, bytes_accessed=4 << 20, transcendentals=0),
        name="dispatch",
    )(at, tokens, routes_t)


def round_kernel(gain_ref, gate_ref, up_ref, out_ref):
    diagonal = iota((64, 64), 0) == iota((64, 64), 1)
    gain = jnp.sum(jnp.where(diagonal, gain_ref[...], 0.0), axis=1, keepdims=True)
    out_ref[:, 0] = (gate_ref[...] * gain[None]).astype(BF)
    out_ref[:, 1] = (up_ref[...] * gain[None]).astype(BF)


def round_both(gain, gate, up):
    block = pl.BlockSpec((8, 64, 128), lambda i: (i, 0, 0))
    return pl.pallas_call(
        round_kernel,
        out_shape=jax.ShapeDtypeStruct((EXPERTS, 2, 64, 128), BF),
        grid=(EXPERTS // 8,),
        in_specs=[pl.BlockSpec((1, 64), lambda i: (0, 0)), block, block],
        out_specs=pl.BlockSpec((8, 2, 64, 128), lambda i: (i, 0, 0, 0)),
        compiler_params=pltpu.CompilerParams(vmem_limit_bytes=60 << 20),
        cost_estimate=pl.CostEstimate(flops=10**7, bytes_accessed=3 << 20, transcendentals=0),
        name="round_both",
    )(gain.reshape(1, 64), gate, up)


WAYS = 10
HALF = 16


def ffn_kernel(block_ref, *refs):
    both_refs, single_refs = refs[:WAYS], refs[WAYS : 2 * WAYS]
    out_ref, *sample_refs = refs[2 * WAYS : 2 * WAYS + 4]
    weight_ref, rows_ref, hidden_ref, sems, sample_sems = refs[2 * WAYS + 4 :]
    places = []
    for side in range(2):
        at = 4 * side
        places += [(at, slice(None)), (at + 1, slice(None)), (at + 2, slice(None))]
        places += [(at + 3, slice(0, HALF)), (at + 3, slice(HALF, None))]
    copies = {}
    for i, (at, part) in enumerate(places):
        for n in range(3):
            source = both_refs[i].at[:, n] if n < 2 else single_refs[i]
            target = weight_ref.at[n, at, part]
            copies[n, i] = pltpu.make_async_copy(source, target, sems.at[n, i])
            copies[n, i].start()

    rows_ref[0:TOK, :] = block_ref[:, :D]
    tail = block_ref[:, D:]
    out_row = iota((64, TOK), 0)
    in_row = iota((64, TOK), 1)
    for j in range(4):
        pick = flag(
            jnp.logical_and(out_row // 2 == in_row // 8, in_row % 8 == 2 * j + out_row % 2)
        )
        rows_ref[TOK : TOK + 64, j * 512 : (j + 1) * 512] = dot(pick, tail).astype(BF)

    def wide(n, blocks, part=slice(None)):
        return jnp.concatenate(
            [weight_ref[n, i, part].reshape(-1, 128) for i in blocks], axis=1
        )

    kept = []

    def keep(n):
        kept.append(
            pltpu.make_async_copy(weight_ref.at[n, 0], sample_refs[n], sample_sems.at[n])
        )
        kept[n].start()

    for pair in range(4):
        for i, (at, _) in enumerate(places):
            if at // 2 == pair:
                copies[0, i].wait()
                copies[1, i].wait()
        blocks = (2 * pair, 2 * pair + 1)
        gate = dot(rows_ref[...], wide(0, blocks))
        up = dot(rows_ref[...], wide(1, blocks))
        hidden = gate / (1.0 + jnp.exp(-gate)) * up
        hidden_ref[:, pair * 256 : (pair + 1) * 256] = hidden.astype(BF)
        if pair == 0:
            keep(0)
            keep(1)

    for i in range(WAYS):
        copies[2, i].wait()
    keep(2)
    out_row = iota((TOK, 64), 0)
    in_row = iota((TOK, 64), 1)
    picks = [
        flag(jnp.logical_and(in_row // 2 == out_row // 8, out_row % 8 == 2 * j + in_row % 2))
        for j in range(4)
    ]
    for x in range(NX):
        result = dot_t(hidden_ref[...], wide(2, range(8), slice(x * 8, (x + 1) * 8)))
        result = result.astype(BF)
        packed = jnp.zeros((TOK, 128), F32)
        for j in range(4):
            packed = packed + dot(picks[j], result[TOK:, j * 128 : (j + 1) * 128])
        out_ref[:, x, :, 0:512] = result[:TOK].reshape(EXPERTS, 8, 512)
        out_ref[:, x, :, 512:640] = packed.astype(BF).reshape(EXPERTS, 8, 128)
    for copy in kept:
        copy.wait()


def ffn(block, both, single):
    sample = jax.ShapeDtypeStruct((EXPERTS, 64, 128), BF)
    return pl.pallas_call(
        ffn_kernel,
        out_shape=(jax.ShapeDtypeStruct((EXPERTS, NX, 8, 640), BF), sample, sample, sample),
        in_specs=[VMEM] + [HBM] * (2 * WAYS),
        out_specs=(VMEM, HBM, HBM, HBM),
        scratch_shapes=[
            pltpu.VMEM((3, 8, EXPERTS, 64, 128), BF),
            pltpu.VMEM((TOK + 64, D), BF),
            pltpu.VMEM((TOK + 64, FF), BF),
            pltpu.SemaphoreType.DMA((3, WAYS)),
            pltpu.SemaphoreType.DMA((3,)),
        ],
        compiler_params=pltpu.CompilerParams(vmem_limit_bytes=52 << 20),
        cost_estimate=pl.CostEstimate(
            flops=6 * 320 * D * FF, bytes_accessed=16 << 20, transcendentals=320 * FF
        ),
        name="ffn",
    )(block, *both, *single)


def mixing_kernel(core_ref, routes_ref, weights_ref, first_ref, last_ref):
    core = core_ref[0]
    expert = iota((TOK, EXPERTS), 1)
    member = jnp.zeros((TOK, EXPERTS), F32)
    weight = jnp.zeros((TOK, EXPERTS), F32)
    for k in range(routes_ref.shape[1]):
        same = routes_ref[:, k : k + 1] == expert
        member = member + jnp.where(same, 1.0, 0.0)
        weight = weight + jnp.where(same, weights_ref[:, k : k + 1], 0.0)
    earlier = flag(iota((TOK, TOK), 1) < iota((TOK, TOK), 0))
    position = dot(earlier, member.astype(BF))
    slot = jnp.where(member > 0.0, position, -1.0).astype(BF)
    spread = flag(iota((EXPERTS, LANES), 1) // (NX * 8) == iota((EXPERTS, LANES), 0))
    slots = dot(slot, spread)
    wide = dot(weight.astype(BF), spread)
    lane = iota((TOK, LANES), 1)
    start = ((lane // 8) % NX * NC + core) * SHARE
    first = slots == (start + lane % 8).astype(F32)
    last = slots == (start + 8 + lane % 2).astype(F32)
    first_ref[...] = jnp.where(first, wide, 0.0).astype(BF)
    last_ref[...] = jnp.where(last, wide, 0.0).astype(BF)


LANES = EXPERTS * NX * 8


def mixing(routes, route_weights, core):
    shape = jax.ShapeDtypeStruct((TOK, LANES), BF)
    return pl.pallas_call(
        mixing_kernel,
        out_shape=(shape, shape),
        in_specs=[SMEM, VMEM, VMEM],
        out_specs=(VMEM, VMEM),
        compiler_params=pltpu.CompilerParams(vmem_limit_bytes=24 << 20),
        cost_estimate=pl.CostEstimate(flops=10**9, bytes_accessed=4 << 20, transcendentals=0),
        name="mixing",
    )(core, routes, route_weights)


def combine_kernel(
    core_ref, back_ref, first_hbm, last_hbm, own_ref, other_ref, first_ref, last_ref, sems
):
    core = core_ref[0]
    copies = [
        pltpu.make_async_copy(source, target, sems.at[i])
        for i, (source, target) in enumerate(
            ((first_hbm, first_ref), (last_hbm, last_ref))
        )
    ]
    for copy in copies:
        copy.start()
    copies[0].wait()
    total = dot(first_ref[...], back_ref[:, 0:512])
    tail = back_ref[:, 512:640]
    lane = iota((TOK, LANES), 1)
    copies[1].wait()
    last = last_ref[...]
    pieces = []
    for j in range(4):
        mine = lane % 8 // 2 == j
        pieces.append(dot(jnp.where(mine, last, jnp.zeros_like(last)), tail))
    total = total + jnp.concatenate(pieces, axis=1)
    left, right = total[:, :256], total[:, 256:]
    own_ref[...] = jnp.where(core == 0, left, right)
    other_ref[...] = jnp.where(core == 0, right, left).astype(BF)


def combine(back, mix, core):
    return pl.pallas_call(
        combine_kernel,
        out_shape=(
            jax.ShapeDtypeStruct((TOK, 256), F32),
            jax.ShapeDtypeStruct((TOK, 256), BF),
        ),
        in_specs=[SMEM, VMEM, HBM, HBM],
        out_specs=(VMEM, VMEM),
        scratch_shapes=[
            pltpu.VMEM((TOK, LANES), BF),
            pltpu.VMEM((TOK, LANES), BF),
            pltpu.SemaphoreType.DMA((2,)),
        ],
        compiler_params=pltpu.CompilerParams(vmem_limit_bytes=24 << 20),
        cost_estimate=pl.CostEstimate(flops=10**9, bytes_accessed=4 << 20, transcendentals=0),
        name="combine",
    )(core, back, *mix)


Z_ORDER = (0, 4, 2, 6, 1, 5, 3, 7)


def shared_kernel(at_ref, normed_ref, *refs):
    block_refs, terms_ref, common_refs = refs[:NY], refs[NY], refs[NY + 1 :]
    z, y = at_ref[0], at_ref[1]
    for dy in range(NY):
        for dz in range(NZ):
            row = ((z + Z_ORDER[dz]) % NZ * NY + (y + dy) % NY) * 64
            part = pl.ds(pl.multiple_of(row, 64), 64)
            for n in range(3):
                common_refs[n][part, :] = block_refs[dy][dz, :, n * 128 : (n + 1) * 128]
    normed = normed_ref[...]
    both = jnp.concatenate([common_refs[0][...], common_refs[1][...]], axis=1)
    act = dot(normed, both)
    gate, up = act[:, 0:128], act[:, 128:256]
    hidden = (gate / (1.0 + jnp.exp(-gate)) * up).astype(BF)
    for n in range(NX * NC):
        terms_ref[n] = dot_t(hidden, common_refs[2][n * 256 : (n + 1) * 256, :]).astype(BF)


def shared_expert(normed, blocks, at):
    shape = jax.ShapeDtypeStruct((D, 128), BF)
    return pl.pallas_call(
        shared_kernel,
        out_shape=(jax.ShapeDtypeStruct((NX * NC, TOK, 256), BF), shape, shape, shape),
        in_specs=[SMEM] + [VMEM] * (1 + NY),
        out_specs=(VMEM,) * 4,
        compiler_params=pltpu.CompilerParams(vmem_limit_bytes=24 << 20),
        cost_estimate=pl.CostEstimate(
            flops=6 * TOK * D * 128, bytes_accessed=6 << 20, transcendentals=TOK * 128
        ),
        name="shared_expert",
    )(at, normed, *blocks)


def exchange(array, axes):
    return lax.all_to_all(array, axes, split_axis=0, concat_axis=0, tiled=True)


def after(*arrays):
    return lax.optimization_barrier(arrays)


def to_neighbours(rows):
    return shift(rows, "x", NX, 1), shift(rows, "x", NX, -1)


def to_opposite(near):
    return shift(near[0][:HALF], "x", NX, 1), shift(near[1][HALF:], "x", NX, -1)


def layer(
    tokens,
    routes,
    route_weights,
    norm_gain,
    expert_gate,
    expert_up,
    expert_down,
    shared_gate,
    shared_up,
    shared_down,
):
    z, y, x, c = (lax.axis_index(a).astype(jnp.int32) for a in FS + TP)
    at = (x * NC + c).reshape(1)
    core = c.reshape(1)

    shared = jnp.concatenate(
        [
            (shared_gate * norm_gain[:, None]).astype(BF),
            (shared_up * norm_gain[:, None]).astype(BF),
            shared_down.astype(BF),
        ],
        axis=1,
    )
    column = shared[None]
    for k in (4, 2, 1):
        column = jnp.concatenate([column, shift(column, "z", NZ, -k)])
    blocks = [column] + [shift(column, "y", NY, -k) for k in range(1, NY)]

    both_in = round_both(norm_gain, expert_gate, expert_up)
    both_in, expert_down = after(both_in, expert_down)
    down_in = expert_down.astype(BF)
    packed, normed = dispatch(tokens, routes.T, at)

    both_rows = exchange(both_in, FS)

    down_in, both_rows = after(down_in, both_rows)
    down_rows = exchange(down_in, FS)
    both_near = to_neighbours(both_rows)

    packed, down_rows = after(packed, down_rows)
    block = exchange(packed.reshape(EXPERTS, 8, D + 512), FS).reshape(TOK, D + 512)
    both_far = to_opposite(both_near)
    down_near = to_neighbours(down_rows)
    down_far = to_opposite(down_near)
    both_all = [both_rows, *both_near, *both_far]
    down_all = [down_rows, *down_near, *down_far]
    both_all += [shift(piece, "c", NC, 1) for piece in both_all]
    down_all += [shift(piece, "c", NC, 1) for piece in down_all]

    shared_terms, common_gate, common_up, common_down = shared_expert(
        normed, blocks, jnp.stack([z, y])
    )
    shared_sum = lax.psum_scatter(shared_terms, TP, scatter_dimension=0, tiled=True)[0]

    results, sample_gate, sample_up, sample_down = ffn(block, both_all, down_all)
    mix = mixing(routes, route_weights, core)
    back = exchange(results.reshape(EXPERTS * NX, 8, 640), ("z", "y", "x"))
    own, other = combine(back.reshape(EXPERTS * NX * 8, 640), mix, core)
    other = shift(other, "c", NC, 1)
    layer_output = (own + other.astype(F32) + shared_sum.astype(F32)).astype(BF)
    return (
        layer_output,
        sample_gate.reshape(1, D, 128),
        sample_up.reshape(1, D, 128),
        sample_down.reshape(1, D, 128),
        common_gate,
        common_up,
        common_down,
    )


def solution(mesh):
    mesh = Mesh(mesh.devices.reshape(NZ, NY, NX, NC), FS + TP)
    return jax.shard_map(
        layer,
        mesh=mesh,
        in_specs=(
            P(FS, None),
            P(FS, None),
            P(FS, None),
            P(FS),
            P(None, FS, TP),
            P(None, FS, TP),
            P(None, FS, TP),
            P(FS, TP),
            P(FS, TP),
            P(FS, TP),
        ),
        out_specs=(
            P(FS, TP),
            P(FS, None, TP),
            P(FS, None, TP),
            P(FS, None, TP),
            P(None, TP),
            P(None, TP),
            P(None, TP),
        ),
        check_vma=False,
    )
```

```python
import jax
import jax.numpy as jnp
from jax import lax
from jax.experimental import pallas as pl
from jax.experimental.pallas import tpu as pltpu
from jax.sharding import Mesh
from jax.sharding import PartitionSpec as P

EPSILON = 1e-06
FS = ("z", "y")
TP = ("x", "c")
NZ, NY, NX, NC = 8, 4, 4, 2
EXPERTS = 32
TOK = 256
D = 2048
FF = 1024
SHARE = 10
BF = jnp.bfloat16
F32 = jnp.float32


def iota(shape, dim):
    return lax.broadcasted_iota(jnp.int32, shape, dim)


def dot(a, b):
    return jnp.dot(a, b, preferred_element_type=F32)


def dot_t(a, b):
    return lax.dot_general(a, b, (((1,), (1,)), ((), ())), preferred_element_type=F32)


def flag(condition):
    return jnp.where(condition, 1.0, 0.0).astype(BF)


def shift(array, axis, size, by):
    return lax.ppermute(array, axis, [(i, (i + by) % size) for i in range(size)])


VMEM = pl.BlockSpec(memory_space=pltpu.VMEM)
SMEM = pl.BlockSpec(memory_space=pltpu.SMEM)
HBM = pl.BlockSpec(memory_space=pltpu.HBM)


def dispatch_kernel(at_ref, tokens_ref, routes_ref, packed_ref, normed_ref):
    base = (at_ref[0] * SHARE).astype(F32)
    values = tokens_ref[...].astype(F32)
    scale = lax.rsqrt(jnp.mean(values * values, axis=-1, keepdims=True) + EPSILON)
    normed = (values * scale).astype(BF)
    normed_ref[...] = normed
    expert = iota((EXPERTS, TOK), 0)
    member = jnp.zeros((EXPERTS, TOK), F32)
    for k in range(routes_ref.shape[0]):
        member = member + jnp.where(routes_ref[k : k + 1, :] == expert, 1.0, 0.0)
    earlier = flag(iota((TOK, TOK), 0) < iota((TOK, TOK), 1))
    position = dot(member.astype(BF), earlier)
    slot = jnp.where(member > 0.0, position, -1.0).astype(BF)
    row = iota((TOK, EXPERTS), 0)
    spread = flag(row // 8 == iota((TOK, EXPERTS), 1))
    slots = dot(spread, slot) - base
    inner = iota((TOK, TOK), 0) % 8
    first = flag(slots == inner.astype(F32))
    packed_ref[:, :D] = dot(first, normed).astype(BF)
    last = slots == (8 + inner % 2).astype(F32)
    tail = jnp.zeros((TOK, 512), F32)
    for j in range(4):
        pick = flag(jnp.logical_and(last, inner // 2 == j))
        tail = tail + dot(pick, normed[:, j * 512 : (j + 1) * 512])
    packed_ref[:, D:] = tail.astype(BF)


def dispatch(tokens, routes_t, at):
    return pl.pallas_call(
        dispatch_kernel,
        out_shape=(
            jax.ShapeDtypeStruct((TOK, D + 512), BF),
            jax.ShapeDtypeStruct((TOK, D), BF),
        ),
        in_specs=[SMEM, VMEM, VMEM],
        out_specs=(VMEM, VMEM),
        compiler_params=pltpu.CompilerParams(vmem_limit_bytes=24 << 20),
        cost_estimate=pl.CostEstimate(flops=10**9, bytes_accessed=4 << 20, transcendentals=0),
        name="dispatch",
    )(at, tokens, routes_t)


def round_kernel(gain_ref, gate_ref, up_ref, out_ref):
    diagonal = iota((64, 64), 0) == iota((64, 64), 1)
    gain = jnp.sum(jnp.where(diagonal, gain_ref[...], 0.0), axis=1, keepdims=True)
    out_ref[:, 0] = (gate_ref[...] * gain[None]).astype(BF)
    out_ref[:, 1] = (up_ref[...] * gain[None]).astype(BF)


def round_both(gain, gate, up):
    block = pl.BlockSpec((8, 64, 128), lambda i: (i, 0, 0))
    return pl.pallas_call(
        round_kernel,
        out_shape=jax.ShapeDtypeStruct((EXPERTS, 2, 64, 128), BF),
        grid=(EXPERTS // 8,),
        in_specs=[pl.BlockSpec((1, 64), lambda i: (0, 0)), block, block],
        out_specs=pl.BlockSpec((8, 2, 64, 128), lambda i: (i, 0, 0, 0)),
        compiler_params=pltpu.CompilerParams(vmem_limit_bytes=60 << 20),
        cost_estimate=pl.CostEstimate(flops=10**7, bytes_accessed=3 << 20, transcendentals=0),
        name="round_both",
    )(gain.reshape(1, 64), gate, up)


WAYS = 10
HALF = 16


def ffn_kernel(block_ref, *refs):
    both_refs, single_refs = refs[:WAYS], refs[WAYS : 2 * WAYS]
    out_ref, *sample_refs = refs[2 * WAYS : 2 * WAYS + 4]
    weight_ref, rows_ref, hidden_ref, sems, sample_sems = refs[2 * WAYS + 4 :]
    places = []
    for side in range(2):
        at = 4 * side
        places += [(at, slice(None)), (at + 1, slice(None)), (at + 2, slice(None))]
        places += [(at + 3, slice(0, HALF)), (at + 3, slice(HALF, None))]
    copies = {}
    for i, (at, part) in enumerate(places):
        for n in range(3):
            source = both_refs[i].at[:, n] if n < 2 else single_refs[i]
            target = weight_ref.at[n, at, part]
            copies[n, i] = pltpu.make_async_copy(source, target, sems.at[n, i])
            copies[n, i].start()

    rows_ref[0:TOK, :] = block_ref[:, :D]
    tail = block_ref[:, D:]
    out_row = iota((64, TOK), 0)
    in_row = iota((64, TOK), 1)
    for j in range(4):
        pick = flag(
            jnp.logical_and(out_row // 2 == in_row // 8, in_row % 8 == 2 * j + out_row % 2)
        )
        rows_ref[TOK : TOK + 64, j * 512 : (j + 1) * 512] = dot(pick, tail).astype(BF)

    def wide(n, blocks, part=slice(None)):
        return jnp.concatenate(
            [weight_ref[n, i, part].reshape(-1, 128) for i in blocks], axis=1
        )

    kept = []

    def keep(n):
        kept.append(
            pltpu.make_async_copy(weight_ref.at[n, 0], sample_refs[n], sample_sems.at[n])
        )
        kept[n].start()

    for pair in range(4):
        for i, (at, _) in enumerate(places):
            if at // 2 == pair:
                copies[0, i].wait()
                copies[1, i].wait()
        blocks = (2 * pair, 2 * pair + 1)
        gate = dot(rows_ref[...], wide(0, blocks))
        up = dot(rows_ref[...], wide(1, blocks))
        hidden = gate / (1.0 + jnp.exp(-gate)) * up
        hidden_ref[:, pair * 256 : (pair + 1) * 256] = hidden.astype(BF)
        if pair == 0:
            keep(0)
            keep(1)

    for i in range(WAYS):
        copies[2, i].wait()
    keep(2)
    out_row = iota((TOK, 64), 0)
    in_row = iota((TOK, 64), 1)
    picks = [
        flag(jnp.logical_and(in_row // 2 == out_row // 8, out_row % 8 == 2 * j + in_row % 2))
        for j in range(4)
    ]
    for x in range(NX):
        result = dot_t(hidden_ref[...], wide(2, range(8), slice(x * 8, (x + 1) * 8)))
        result = result.astype(BF)
        packed = jnp.zeros((TOK, 128), F32)
        for j in range(4):
            packed = packed + dot(picks[j], result[TOK:, j * 128 : (j + 1) * 128])
        out_ref[:, x, :, 0:512] = result[:TOK].reshape(EXPERTS, 8, 512)
        out_ref[:, x, :, 512:640] = packed.astype(BF).reshape(EXPERTS, 8, 128)
    for copy in kept:
        copy.wait()


def ffn(block, both, single):
    sample = jax.ShapeDtypeStruct((EXPERTS, 64, 128), BF)
    return pl.pallas_call(
        ffn_kernel,
        out_shape=(jax.ShapeDtypeStruct((EXPERTS, NX, 8, 640), BF), sample, sample, sample),
        in_specs=[VMEM] + [HBM] * (2 * WAYS),
        out_specs=(VMEM, HBM, HBM, HBM),
        scratch_shapes=[
            pltpu.VMEM((3, 8, EXPERTS, 64, 128), BF),
            pltpu.VMEM((TOK + 64, D), BF),
            pltpu.VMEM((TOK + 64, FF), BF),
            pltpu.SemaphoreType.DMA((3, WAYS)),
            pltpu.SemaphoreType.DMA((3,)),
        ],
        compiler_params=pltpu.CompilerParams(vmem_limit_bytes=52 << 20),
        cost_estimate=pl.CostEstimate(
            flops=6 * 320 * D * FF, bytes_accessed=16 << 20, transcendentals=320 * FF
        ),
        name="ffn",
    )(block, *both, *single)


def mixing_kernel(core_ref, routes_ref, weights_ref, first_ref, last_ref):
    core = core_ref[0]
    expert = iota((TOK, EXPERTS), 1)
    member = jnp.zeros((TOK, EXPERTS), F32)
    weight = jnp.zeros((TOK, EXPERTS), F32)
    for k in range(routes_ref.shape[1]):
        same = routes_ref[:, k : k + 1] == expert
        member = member + jnp.where(same, 1.0, 0.0)
        weight = weight + jnp.where(same, weights_ref[:, k : k + 1], 0.0)
    earlier = flag(iota((TOK, TOK), 1) < iota((TOK, TOK), 0))
    position = dot(earlier, member.astype(BF))
    slot = jnp.where(member > 0.0, position, -1.0).astype(BF)
    spread = flag(iota((EXPERTS, LANES), 1) // (NX * 8) == iota((EXPERTS, LANES), 0))
    slots = dot(slot, spread)
    wide = dot(weight.astype(BF), spread)
    lane = iota((TOK, LANES), 1)
    start = ((lane // 8) % NX * NC + core) * SHARE
    first = slots == (start + lane % 8).astype(F32)
    last = slots == (start + 8 + lane % 2).astype(F32)
    first_ref[...] = jnp.where(first, wide, 0.0).astype(BF)
    last_ref[...] = jnp.where(last, wide, 0.0).astype(BF)


LANES = EXPERTS * NX * 8


def mixing(routes, route_weights, core):
    shape = jax.ShapeDtypeStruct((TOK, LANES), BF)
    return pl.pallas_call(
        mixing_kernel,
        out_shape=(shape, shape),
        in_specs=[SMEM, VMEM, VMEM],
        out_specs=(VMEM, VMEM),
        compiler_params=pltpu.CompilerParams(vmem_limit_bytes=24 << 20),
        cost_estimate=pl.CostEstimate(flops=10**9, bytes_accessed=4 << 20, transcendentals=0),
        name="mixing",
    )(core, routes, route_weights)


def combine_kernel(
    core_ref, back_ref, first_hbm, last_hbm, own_ref, other_ref, first_ref, last_ref, sems
):
    core = core_ref[0]
    copies = [
        pltpu.make_async_copy(source, target, sems.at[i])
        for i, (source, target) in enumerate(
            ((first_hbm, first_ref), (last_hbm, last_ref))
        )
    ]
    for copy in copies:
        copy.start()
    copies[0].wait()
    total = dot(first_ref[...], back_ref[:, 0:512])
    tail = back_ref[:, 512:640]
    lane = iota((TOK, LANES), 1)
    copies[1].wait()
    last = last_ref[...]
    pieces = []
    for j in range(4):
        mine = lane % 8 // 2 == j
        pieces.append(dot(jnp.where(mine, last, jnp.zeros_like(last)), tail))
    total = total + jnp.concatenate(pieces, axis=1)
    left, right = total[:, :256], total[:, 256:]
    own_ref[...] = jnp.where(core == 0, left, right)
    other_ref[...] = jnp.where(core == 0, right, left).astype(BF)


def combine(back, mix, core):
    return pl.pallas_call(
        combine_kernel,
        out_shape=(
            jax.ShapeDtypeStruct((TOK, 256), F32),
            jax.ShapeDtypeStruct((TOK, 256), BF),
        ),
        in_specs=[SMEM, VMEM, HBM, HBM],
        out_specs=(VMEM, VMEM),
        scratch_shapes=[
            pltpu.VMEM((TOK, LANES), BF),
            pltpu.VMEM((TOK, LANES), BF),
            pltpu.SemaphoreType.DMA((2,)),
        ],
        compiler_params=pltpu.CompilerParams(vmem_limit_bytes=24 << 20),
        cost_estimate=pl.CostEstimate(flops=10**9, bytes_accessed=4 << 20, transcendentals=0),
        name="combine",
    )(core, back, *mix)


def shared_kernel(normed_ref, common_ref, terms_ref, *common_refs):
    for n in range(3):
        common_refs[n][...] = common_ref[:, n * 128 : (n + 1) * 128]
    act = dot(normed_ref[...], common_ref[:, 0:256])
    gate, up = act[:, 0:128], act[:, 128:256]
    hidden = (gate / (1.0 + jnp.exp(-gate)) * up).astype(BF)
    for n in range(NX * NC):
        terms_ref[n] = dot_t(hidden, common_ref[n * 256 : (n + 1) * 256, 256:384]).astype(BF)


def shared_expert(normed, common):
    shape = jax.ShapeDtypeStruct((D, 128), BF)
    return pl.pallas_call(
        shared_kernel,
        out_shape=(jax.ShapeDtypeStruct((NX * NC, TOK, 256), BF), shape, shape, shape),
        in_specs=[VMEM] * 2,
        out_specs=(VMEM,) * 4,
        compiler_params=pltpu.CompilerParams(vmem_limit_bytes=24 << 20),
        cost_estimate=pl.CostEstimate(
            flops=6 * TOK * D * 128, bytes_accessed=6 << 20, transcendentals=TOK * 128
        ),
        name="shared_expert",
    )(normed, common)


def exchange(array, axes):
    return lax.all_to_all(array, axes, split_axis=0, concat_axis=0, tiled=True)


def after(*arrays):
    return lax.optimization_barrier(arrays)


def to_neighbours(rows):
    return shift(rows, "x", NX, 1), shift(rows, "x", NX, -1)


def to_opposite(near):
    return shift(near[0][:HALF], "x", NX, 1), shift(near[1][HALF:], "x", NX, -1)


def layer(
    tokens,
    routes,
    route_weights,
    norm_gain,
    expert_gate,
    expert_up,
    expert_down,
    shared_gate,
    shared_up,
    shared_down,
):
    x, c = (lax.axis_index(a).astype(jnp.int32) for a in TP)
    at = (x * NC + c).reshape(1)
    core = c.reshape(1)

    shared = jnp.concatenate(
        [
            (shared_gate * norm_gain[:, None]).astype(BF),
            (shared_up * norm_gain[:, None]).astype(BF),
            shared_down.astype(BF),
        ],
        axis=1,
    )
    common = lax.all_gather(shared, FS, axis=0, tiled=True)

    both_in = round_both(norm_gain, expert_gate, expert_up)
    both_in, expert_down = after(both_in, expert_down)
    down_in = expert_down.astype(BF)
    packed, normed = dispatch(tokens, routes.T, at)

    both_rows = exchange(both_in, FS)

    down_in, both_rows = after(down_in, both_rows)
    down_rows = exchange(down_in, FS)
    both_near = to_neighbours(both_rows)

    packed, down_rows = after(packed, down_rows)
    block = exchange(packed.reshape(EXPERTS, 8, D + 512), FS).reshape(TOK, D + 512)
    both_far = to_opposite(both_near)
    down_near = to_neighbours(down_rows)
    down_far = to_opposite(down_near)
    both_all = [both_rows, *both_near, *both_far]
    down_all = [down_rows, *down_near, *down_far]
    both_all += [shift(piece, "c", NC, 1) for piece in both_all]
    down_all += [shift(piece, "c", NC, 1) for piece in down_all]

    shared_terms, common_gate, common_up, common_down = shared_expert(normed, common)
    shared_sum = lax.psum_scatter(shared_terms, TP, scatter_dimension=0, tiled=True)[0]

    results, sample_gate, sample_up, sample_down = ffn(block, both_all, down_all)
    mix = mixing(routes, route_weights, core)
    back = exchange(results.reshape(EXPERTS * NX, 8, 640), ("z", "y", "x"))
    own, other = combine(back.reshape(EXPERTS * NX * 8, 640), mix, core)
    other = shift(other, "c", NC, 1)
    layer_output = (own + other.astype(F32) + shared_sum.astype(F32)).astype(BF)
    return (
        layer_output,
        sample_gate.reshape(1, D, 128),
        sample_up.reshape(1, D, 128),
        sample_down.reshape(1, D, 128),
        common_gate,
        common_up,
        common_down,
    )


def solution(mesh):
    mesh = Mesh(mesh.devices.reshape(NZ, NY, NX, NC), FS + TP)
    return jax.shard_map(
        layer,
        mesh=mesh,
        in_specs=(
            P(FS, None),
            P(FS, None),
            P(FS, None),
            P(FS),
            P(None, FS, TP),
            P(None, FS, TP),
            P(None, FS, TP),
            P(FS, TP),
            P(FS, TP),
            P(FS, TP),
        ),
        out_specs=(
            P(FS, TP),
            P(FS, None, TP),
            P(FS, None, TP),
            P(FS, None, TP),
            P(None, TP),
            P(None, TP),
            P(None, TP),
        ),
        check_vma=False,
    )
```

```python
import jax
import jax.numpy as jnp
from jax import lax
from jax.experimental import pallas as pl
from jax.experimental.pallas import tpu as pltpu
from jax.sharding import Mesh
from jax.sharding import PartitionSpec as P

EPSILON = 1e-06
FS = ("z", "y")
TP = ("x", "c")
NZ, NY, NX, NC = 8, 4, 4, 2
EXPERTS = 32
TOK = 256
D = 2048
FF = 1024
SHARE = 10
BF = jnp.bfloat16
F32 = jnp.float32


def iota(shape, dim):
    return lax.broadcasted_iota(jnp.int32, shape, dim)


def dot(a, b):
    return jnp.dot(a, b, preferred_element_type=F32)


def dot_t(a, b):
    return lax.dot_general(a, b, (((1,), (1,)), ((), ())), preferred_element_type=F32)


def flag(condition):
    return jnp.where(condition, 1.0, 0.0).astype(BF)


def shift(array, axis, size, by):
    return lax.ppermute(array, axis, [(i, (i + by) % size) for i in range(size)])


VMEM = pl.BlockSpec(memory_space=pltpu.VMEM)
SMEM = pl.BlockSpec(memory_space=pltpu.SMEM)
HBM = pl.BlockSpec(memory_space=pltpu.HBM)


def dispatch_kernel(at_ref, tokens_ref, routes_ref, packed_ref, normed_ref):
    base = (at_ref[0] * SHARE).astype(F32)
    values = tokens_ref[...].astype(F32)
    scale = lax.rsqrt(jnp.mean(values * values, axis=-1, keepdims=True) + EPSILON)
    normed = (values * scale).astype(BF)
    normed_ref[...] = normed
    expert = iota((EXPERTS, TOK), 0)
    member = jnp.zeros((EXPERTS, TOK), F32)
    for k in range(routes_ref.shape[0]):
        member = member + jnp.where(routes_ref[k : k + 1, :] == expert, 1.0, 0.0)
    earlier = flag(iota((TOK, TOK), 0) < iota((TOK, TOK), 1))
    position = dot(member.astype(BF), earlier)
    slot = jnp.where(member > 0.0, position, -1.0).astype(BF)
    row = iota((TOK, EXPERTS), 0)
    spread = flag(row // 8 == iota((TOK, EXPERTS), 1))
    slots = dot(spread, slot) - base
    inner = iota((TOK, TOK), 0) % 8
    first = flag(slots == inner.astype(F32))
    packed_ref[:, :D] = dot(first, normed).astype(BF)
    last = slots == (8 + inner % 2).astype(F32)
    tail = jnp.zeros((TOK, 512), F32)
    for j in range(4):
        pick = flag(jnp.logical_and(last, inner // 2 == j))
        tail = tail + dot(pick, normed[:, j * 512 : (j + 1) * 512])
    packed_ref[:, D:] = tail.astype(BF)


def dispatch(tokens, routes_t, at):
    return pl.pallas_call(
        dispatch_kernel,
        out_shape=(
            jax.ShapeDtypeStruct((TOK, D + 512), BF),
            jax.ShapeDtypeStruct((TOK, D), BF),
        ),
        in_specs=[SMEM, VMEM, VMEM],
        out_specs=(VMEM, VMEM),
        compiler_params=pltpu.CompilerParams(vmem_limit_bytes=24 << 20),
        cost_estimate=pl.CostEstimate(flops=10**9, bytes_accessed=4 << 20, transcendentals=0),
        name="dispatch",
    )(at, tokens, routes_t)


def round_kernel(gain_ref, gate_ref, up_ref, out_ref):
    diagonal = iota((64, 64), 0) == iota((64, 64), 1)
    gain = jnp.sum(jnp.where(diagonal, gain_ref[...], 0.0), axis=1, keepdims=True)
    out_ref[:, 0] = (gate_ref[...] * gain[None]).astype(BF)
    out_ref[:, 1] = (up_ref[...] * gain[None]).astype(BF)


def round_both(gain, gate, up):
    block = pl.BlockSpec((8, 64, 128), lambda i: (i, 0, 0))
    return pl.pallas_call(
        round_kernel,
        out_shape=jax.ShapeDtypeStruct((EXPERTS, 2, 64, 128), BF),
        grid=(EXPERTS // 8,),
        in_specs=[pl.BlockSpec((1, 64), lambda i: (0, 0)), block, block],
        out_specs=pl.BlockSpec((8, 2, 64, 128), lambda i: (i, 0, 0, 0)),
        compiler_params=pltpu.CompilerParams(vmem_limit_bytes=60 << 20),
        cost_estimate=pl.CostEstimate(flops=10**7, bytes_accessed=3 << 20, transcendentals=0),
        name="round_both",
    )(gain.reshape(1, 64), gate, up)


WAYS = 10
HALF = 16


def ffn_kernel(block_ref, *refs):
    both_refs, single_refs = refs[:WAYS], refs[WAYS : 2 * WAYS]
    out_ref, *sample_refs = refs[2 * WAYS : 2 * WAYS + 4]
    weight_ref, rows_ref, hidden_ref, sems, sample_sems = refs[2 * WAYS + 4 :]
    places = []
    for side in range(2):
        at = 4 * side
        places += [(at, slice(None)), (at + 1, slice(None)), (at + 2, slice(None))]
        places += [(at + 3, slice(0, HALF)), (at + 3, slice(HALF, None))]
    copies = {}
    for i, (at, part) in enumerate(places):
        for n in range(3):
            source = both_refs[i].at[:, n] if n < 2 else single_refs[i]
            target = weight_ref.at[n, at, part]
            copies[n, i] = pltpu.make_async_copy(source, target, sems.at[n, i])
            copies[n, i].start()

    rows_ref[0:TOK, :] = block_ref[:, :D]
    tail = block_ref[:, D:]
    out_row = iota((64, TOK), 0)
    in_row = iota((64, TOK), 1)
    for j in range(4):
        pick = flag(
            jnp.logical_and(out_row // 2 == in_row // 8, in_row % 8 == 2 * j + out_row % 2)
        )
        rows_ref[TOK : TOK + 64, j * 512 : (j + 1) * 512] = dot(pick, tail).astype(BF)

    def wide(n, blocks, part=slice(None)):
        return jnp.concatenate(
            [weight_ref[n, i, part].reshape(-1, 128) for i in blocks], axis=1
        )

    kept = []

    def keep(n):
        kept.append(
            pltpu.make_async_copy(weight_ref.at[n, 0], sample_refs[n], sample_sems.at[n])
        )
        kept[n].start()

    for pair in range(4):
        for i, (at, _) in enumerate(places):
            if at // 2 == pair:
                copies[0, i].wait()
                copies[1, i].wait()
        blocks = (2 * pair, 2 * pair + 1)
        gate = dot(rows_ref[...], wide(0, blocks))
        up = dot(rows_ref[...], wide(1, blocks))
        hidden = gate / (1.0 + jnp.exp(-gate)) * up
        hidden_ref[:, pair * 256 : (pair + 1) * 256] = hidden.astype(BF)
        if pair == 0:
            keep(0)
            keep(1)

    for i in range(WAYS):
        copies[2, i].wait()
    keep(2)
    out_row = iota((TOK, 64), 0)
    in_row = iota((TOK, 64), 1)
    packed = jnp.zeros((TOK, 512), F32)
    for j in range(4):
        result = dot_t(hidden_ref[...], wide(2, range(8), slice(j * 8, (j + 1) * 8)))
        result = result.astype(BF)
        pick = jnp.logical_and(in_row // 2 == out_row // 8, out_row % 8 == 2 * j + in_row % 2)
        packed = packed + dot(flag(pick), result[TOK:])
        out_ref[:, j * 512 : (j + 1) * 512] = result[:TOK]
    out_ref[:, D:] = packed.astype(BF)
    for copy in kept:
        copy.wait()


def ffn(block, both, single):
    sample = jax.ShapeDtypeStruct((EXPERTS, 64, 128), BF)
    return pl.pallas_call(
        ffn_kernel,
        out_shape=(jax.ShapeDtypeStruct((TOK, D + 512), BF), sample, sample, sample),
        in_specs=[VMEM] + [HBM] * (2 * WAYS),
        out_specs=(VMEM, HBM, HBM, HBM),
        scratch_shapes=[
            pltpu.VMEM((3, 8, EXPERTS, 64, 128), BF),
            pltpu.VMEM((TOK + 64, D), BF),
            pltpu.VMEM((TOK + 64, FF), BF),
            pltpu.SemaphoreType.DMA((3, WAYS)),
            pltpu.SemaphoreType.DMA((3,)),
        ],
        compiler_params=pltpu.CompilerParams(vmem_limit_bytes=52 << 20),
        cost_estimate=pl.CostEstimate(
            flops=6 * 320 * D * FF, bytes_accessed=16 << 20, transcendentals=320 * FF
        ),
        name="ffn",
    )(block, *both, *single)


def mixing_kernel(at_ref, routes_ref, weights_ref, first_ref, last_ref):
    expert = iota((TOK, EXPERTS), 1)
    member = jnp.zeros((TOK, EXPERTS), F32)
    weight = jnp.zeros((TOK, EXPERTS), F32)
    for k in range(routes_ref.shape[1]):
        same = routes_ref[:, k : k + 1] == expert
        member = member + jnp.where(same, 1.0, 0.0)
        weight = weight + jnp.where(same, weights_ref[:, k : k + 1], 0.0)
    earlier = flag(iota((TOK, TOK), 1) < iota((TOK, TOK), 0))
    position = dot(earlier, member.astype(BF))
    slot = jnp.where(member > 0.0, position, -1.0).astype(BF)
    spread = flag(iota((EXPERTS, LANES), 1) // 8 == iota((EXPERTS, LANES), 0))
    slots = dot(slot, spread)
    wide = dot(weight.astype(BF), spread)
    lane = iota((TOK, LANES), 1)
    start = at_ref[0] * SHARE
    first = slots == (start + lane % 8).astype(F32)
    last = slots == (start + 8 + lane % 2).astype(F32)
    first_ref[...] = jnp.where(first, wide, 0.0).astype(BF)
    last_ref[...] = jnp.where(last, wide, 0.0).astype(BF)


LANES = EXPERTS * 8


def mixing(routes, route_weights, at):
    shape = jax.ShapeDtypeStruct((TOK, LANES), BF)
    return pl.pallas_call(
        mixing_kernel,
        out_shape=(shape, shape),
        in_specs=[SMEM, VMEM, VMEM],
        out_specs=(VMEM, VMEM),
        compiler_params=pltpu.CompilerParams(vmem_limit_bytes=24 << 20),
        cost_estimate=pl.CostEstimate(flops=10**9, bytes_accessed=4 << 20, transcendentals=0),
        name="mixing",
    )(at, routes, route_weights)


def combine_kernel(
    core_ref,
    back_ref,
    first_hbm,
    last_hbm,
    terms_hbm,
    mine_ref,
    other_ref,
    first_ref,
    last_ref,
    terms_ref,
    sems,
):
    core = core_ref[0]
    copies = [
        pltpu.make_async_copy(source, target, sems.at[i])
        for i, (source, target) in enumerate(
            ((first_hbm, first_ref), (last_hbm, last_ref), (terms_hbm, terms_ref))
        )
    ]
    for copy in copies:
        copy.start()
    copies[0].wait()
    copies[1].wait()
    lane = iota((TOK, LANES), 1)
    last = last_ref[...]
    tail = back_ref[:, D:]
    for j in range(NX):
        part = slice(j * 512, (j + 1) * 512)
        pick = jnp.where(lane % 8 // 2 == j, last, jnp.zeros_like(last))
        total = dot(first_ref[...], back_ref[:, part]) + dot(pick, tail)
        if j == 0:
            copies[2].wait()
        total = total + terms_ref[:, part].astype(F32)
        left, right = total[:, :256], total[:, 256:]
        mine_ref[j] = jnp.where(core == 0, left, right)
        other_ref[j] = jnp.where(core == 0, right, left).astype(BF)


def combine(back, mix, terms, core):
    return pl.pallas_call(
        combine_kernel,
        out_shape=(
            jax.ShapeDtypeStruct((NX, TOK, 256), F32),
            jax.ShapeDtypeStruct((NX, TOK, 256), BF),
        ),
        in_specs=[SMEM, VMEM] + [HBM] * 3,
        out_specs=(VMEM, VMEM),
        scratch_shapes=[
            pltpu.VMEM((TOK, LANES), BF),
            pltpu.VMEM((TOK, LANES), BF),
            pltpu.VMEM((TOK, D), BF),
            pltpu.SemaphoreType.DMA((3,)),
        ],
        compiler_params=pltpu.CompilerParams(vmem_limit_bytes=24 << 20),
        cost_estimate=pl.CostEstimate(flops=10**9, bytes_accessed=4 << 20, transcendentals=0),
        name="combine",
    )(core, back, *mix, terms)


def shared_kernel(at_ref, normed_ref, *refs):
    block_refs, terms_ref, common_refs = refs[:NY], refs[NY], refs[NY + 1 :]
    z, y = at_ref[0], at_ref[1]
    for dy in range(NY):
        for dz in range(NZ):
            row = ((z + dz) % NZ * NY + (y + dy) % NY) * 64
            part = pl.ds(pl.multiple_of(row, 64), 64)
            for n in range(3):
                common_refs[n][part, :] = block_refs[dy][dz, :, n * 128 : (n + 1) * 128]
    both = jnp.concatenate([common_refs[0][...], common_refs[1][...]], axis=1)
    act = dot(normed_ref[...], both)
    gate, up = act[:, 0:128], act[:, 128:256]
    hidden = (gate / (1.0 + jnp.exp(-gate)) * up).astype(BF)
    terms_ref[...] = dot_t(hidden, common_refs[2][...]).astype(BF)


def shared_expert(normed, blocks, at):
    shape = jax.ShapeDtypeStruct((D, 128), BF)
    terms = jax.ShapeDtypeStruct((TOK, D), BF)
    return pl.pallas_call(
        shared_kernel,
        out_shape=(terms, shape, shape, shape),
        in_specs=[SMEM] + [VMEM] * (1 + NY),
        out_specs=(VMEM,) * 4,
        compiler_params=pltpu.CompilerParams(vmem_limit_bytes=24 << 20),
        cost_estimate=pl.CostEstimate(
            flops=6 * TOK * D * 128, bytes_accessed=6 << 20, transcendentals=TOK * 128
        ),
        name="shared_expert",
    )(at, normed, *blocks)


def pair_kernel(at_ref, mine_ref, swapped_ref, *out_refs):
    for dx in range(NX):
        x = (at_ref[0] + dx) % NX
        total = mine_ref[x] + swapped_ref[x].astype(F32)
        out_refs[dx][...] = total.astype(BF)


def pair_sum(mine, swapped, at):
    shape = jax.ShapeDtypeStruct((TOK, 256), BF)
    return pl.pallas_call(
        pair_kernel,
        out_shape=(shape,) * NX,
        in_specs=[SMEM, VMEM, VMEM],
        out_specs=(VMEM,) * NX,
        compiler_params=pltpu.CompilerParams(vmem_limit_bytes=8 << 20),
        cost_estimate=pl.CostEstimate(flops=10**6, bytes_accessed=2 << 20, transcendentals=0),
        name="pair_sum",
    )(at, mine, swapped)


def exchange(array, axes):
    return lax.all_to_all(array, axes, split_axis=0, concat_axis=0, tiled=True)


def after(*arrays):
    return lax.optimization_barrier(arrays)


def to_neighbours(rows):
    return shift(rows, "x", NX, 1), shift(rows, "x", NX, -1)


def to_opposite(near):
    return shift(near[0][:HALF], "x", NX, 1), shift(near[1][HALF:], "x", NX, -1)


def layer(
    tokens,
    routes,
    route_weights,
    norm_gain,
    expert_gate,
    expert_up,
    expert_down,
    shared_gate,
    shared_up,
    shared_down,
):
    z, y, x, c = (lax.axis_index(a).astype(jnp.int32) for a in FS + TP)
    at = (x * NC + c).reshape(1)
    core = c.reshape(1)

    shared = jnp.concatenate(
        [
            (shared_gate * norm_gain[:, None]).astype(BF),
            (shared_up * norm_gain[:, None]).astype(BF),
            shared_down.astype(BF),
        ],
        axis=1,
    )
    column = [shared] + [shift(shared, "z", NZ, -k) for k in range(1, NZ)]
    column = jnp.stack(column)
    blocks = [column] + [shift(column, "y", NY, -k) for k in range(1, NY)]

    both_in = round_both(norm_gain, expert_gate, expert_up)
    both_in, expert_down = after(both_in, expert_down)
    down_in = expert_down.astype(BF)
    packed, normed = dispatch(tokens, routes.T, at)

    both_rows = exchange(both_in, FS)

    down_in, both_rows = after(down_in, both_rows)
    down_rows = exchange(down_in, FS)
    both_near = to_neighbours(both_rows)

    packed, down_rows = after(packed, down_rows)
    block = exchange(packed.reshape(EXPERTS, 8, D + 512), FS).reshape(TOK, D + 512)
    both_far = to_opposite(both_near)
    down_near = to_neighbours(down_rows)
    down_far = to_opposite(down_near)
    both_all = [both_rows, *both_near, *both_far]
    down_all = [down_rows, *down_near, *down_far]
    both_all += [shift(piece, "c", NC, 1) for piece in both_all]
    down_all += [shift(piece, "c", NC, 1) for piece in down_all]

    terms, common_gate, common_up, common_down = shared_expert(
        normed, blocks, jnp.stack([z, y])
    )

    results, sample_gate, sample_up, sample_down = ffn(block, both_all, down_all)
    mix = mixing(routes, route_weights, at)
    back = exchange(results.reshape(EXPERTS, 8, D + 512), FS).reshape(TOK, D + 512)
    mine, other = combine(back, mix, terms, core)
    sums = pair_sum(mine, shift(other, "c", NC, 1), x.reshape(1))
    sums = [sums[0]] + [shift(sums[k], "x", NX, k) for k in range(1, NX)]
    layer_output = sum(part.astype(F32) for part in sums).astype(BF)
    return (
        layer_output,
        sample_gate.reshape(1, D, 128),
        sample_up.reshape(1, D, 128),
        sample_down.reshape(1, D, 128),
        common_gate,
        common_up,
        common_down,
    )


def solution(mesh):
    mesh = Mesh(mesh.devices.reshape(NZ, NY, NX, NC), FS + TP)
    return jax.shard_map(
        layer,
        mesh=mesh,
        in_specs=(
            P(FS, None),
            P(FS, None),
            P(FS, None),
            P(FS),
            P(None, FS, TP),
            P(None, FS, TP),
            P(None, FS, TP),
            P(FS, TP),
            P(FS, TP),
            P(FS, TP),
        ),
        out_specs=(
            P(FS, TP),
            P(FS, None, TP),
            P(FS, None, TP),
            P(FS, None, TP),
            P(None, TP),
            P(None, TP),
            P(None, TP),
        ),
        check_vma=False,
    )
```

```python
import jax
import jax.numpy as jnp
from jax import lax
from jax.experimental import pallas as pl
from jax.experimental.pallas import tpu as pltpu
from jax.sharding import Mesh
from jax.sharding import PartitionSpec as P

EPSILON = 1e-06
FS = ("z", "y")
TP = ("x", "c")
NZ, NY, NX, NC = 8, 4, 4, 2
EXPERTS = 32
TOK = 256
D = 2048
FF = 1024
SHARE = 10
BF = jnp.bfloat16
F32 = jnp.float32


def iota(shape, dim):
    return lax.broadcasted_iota(jnp.int32, shape, dim)


def dot(a, b):
    return jnp.dot(a, b, preferred_element_type=F32)


def dot_t(a, b):
    return lax.dot_general(a, b, (((1,), (1,)), ((), ())), preferred_element_type=F32)


def flag(condition):
    return jnp.where(condition, 1.0, 0.0).astype(BF)


def shift(array, axis, size, by):
    return lax.ppermute(array, axis, [(i, (i + by) % size) for i in range(size)])


VMEM = pl.BlockSpec(memory_space=pltpu.VMEM)
SMEM = pl.BlockSpec(memory_space=pltpu.SMEM)
HBM = pl.BlockSpec(memory_space=pltpu.HBM)


def dispatch_kernel(at_ref, tokens_ref, routes_ref, packed_ref, normed_ref):
    base = (at_ref[0] * SHARE).astype(F32)
    values = tokens_ref[...].astype(F32)
    scale = lax.rsqrt(jnp.mean(values * values, axis=-1, keepdims=True) + EPSILON)
    normed = (values * scale).astype(BF)
    normed_ref[...] = normed
    expert = iota((EXPERTS, TOK), 0)
    member = jnp.zeros((EXPERTS, TOK), F32)
    for k in range(routes_ref.shape[0]):
        member = member + jnp.where(routes_ref[k : k + 1, :] == expert, 1.0, 0.0)
    earlier = flag(iota((TOK, TOK), 0) < iota((TOK, TOK), 1))
    position = dot(member.astype(BF), earlier)
    slot = jnp.where(member > 0.0, position, -1.0).astype(BF)
    row = iota((TOK, EXPERTS), 0)
    spread = flag(row // 8 == iota((TOK, EXPERTS), 1))
    slots = dot(spread, slot) - base
    inner = iota((TOK, TOK), 0) % 8
    first = flag(slots == inner.astype(F32))
    packed_ref[:, :D] = dot(first, normed).astype(BF)
    last = slots == (8 + inner % 2).astype(F32)
    tail = jnp.zeros((TOK, 512), F32)
    for j in range(4):
        pick = flag(jnp.logical_and(last, inner // 2 == j))
        tail = tail + dot(pick, normed[:, j * 512 : (j + 1) * 512])
    packed_ref[:, D:] = tail.astype(BF)


def dispatch(tokens, routes_t, at):
    return pl.pallas_call(
        dispatch_kernel,
        out_shape=(
            jax.ShapeDtypeStruct((TOK, D + 512), BF),
            jax.ShapeDtypeStruct((TOK, D), BF),
        ),
        in_specs=[SMEM, VMEM, VMEM],
        out_specs=(VMEM, VMEM),
        compiler_params=pltpu.CompilerParams(vmem_limit_bytes=24 << 20),
        cost_estimate=pl.CostEstimate(flops=10**9, bytes_accessed=4 << 20, transcendentals=0),
        name="dispatch",
    )(at, tokens, routes_t)


def round_kernel(gain_ref, gate_ref, up_ref, out_ref):
    diagonal = iota((64, 64), 0) == iota((64, 64), 1)
    gain = jnp.sum(jnp.where(diagonal, gain_ref[...], 0.0), axis=1, keepdims=True)
    out_ref[:, 0] = (gate_ref[...] * gain[None]).astype(BF)
    out_ref[:, 1] = (up_ref[...] * gain[None]).astype(BF)


def round_both(gain, gate, up):
    block = pl.BlockSpec((8, 64, 128), lambda i: (i, 0, 0))
    return pl.pallas_call(
        round_kernel,
        out_shape=jax.ShapeDtypeStruct((EXPERTS, 2, 64, 128), BF),
        grid=(EXPERTS // 8,),
        in_specs=[pl.BlockSpec((1, 64), lambda i: (0, 0)), block, block],
        out_specs=pl.BlockSpec((8, 2, 64, 128), lambda i: (i, 0, 0, 0)),
        compiler_params=pltpu.CompilerParams(vmem_limit_bytes=60 << 20),
        cost_estimate=pl.CostEstimate(flops=10**7, bytes_accessed=3 << 20, transcendentals=0),
        name="round_both",
    )(gain.reshape(1, 64), gate, up)


WAYS = 10
HALF = 16


def ffn_kernel(block_ref, *refs):
    both_refs, single_refs = refs[:WAYS], refs[WAYS : 2 * WAYS]
    out_ref, *sample_refs = refs[2 * WAYS : 2 * WAYS + 4]
    weight_ref, rows_ref, hidden_ref, sems, sample_sems = refs[2 * WAYS + 4 :]
    places = []
    for side in range(2):
        at = 4 * side
        places += [(at, slice(None)), (at + 1, slice(None)), (at + 2, slice(None))]
        places += [(at + 3, slice(0, HALF)), (at + 3, slice(HALF, None))]
    copies = {}
    for i, (at, part) in enumerate(places):
        for n in range(3):
            source = both_refs[i].at[:, n] if n < 2 else single_refs[i]
            target = weight_ref.at[n, at, part]
            copies[n, i] = pltpu.make_async_copy(source, target, sems.at[n, i])
            copies[n, i].start()

    rows_ref[0:TOK, :] = block_ref[:, :D]
    tail = block_ref[:, D:]
    out_row = iota((64, TOK), 0)
    in_row = iota((64, TOK), 1)
    for j in range(4):
        pick = flag(
            jnp.logical_and(out_row // 2 == in_row // 8, in_row % 8 == 2 * j + out_row % 2)
        )
        rows_ref[TOK : TOK + 64, j * 512 : (j + 1) * 512] = dot(pick, tail).astype(BF)

    def wide(n, blocks, part=slice(None)):
        return jnp.concatenate(
            [weight_ref[n, i, part].reshape(-1, 128) for i in blocks], axis=1
        )

    kept = []

    def keep(n):
        kept.append(
            pltpu.make_async_copy(weight_ref.at[n, 0], sample_refs[n], sample_sems.at[n])
        )
        kept[n].start()

    for pair in range(4):
        for i, (at, _) in enumerate(places):
            if at // 2 == pair:
                copies[0, i].wait()
                copies[1, i].wait()
        blocks = (2 * pair, 2 * pair + 1)
        gate = dot(rows_ref[...], wide(0, blocks))
        up = dot(rows_ref[...], wide(1, blocks))
        hidden = gate / (1.0 + jnp.exp(-gate)) * up
        hidden_ref[:, pair * 256 : (pair + 1) * 256] = hidden.astype(BF)
        if pair == 0:
            keep(0)
            keep(1)

    for i in range(WAYS):
        copies[2, i].wait()
    keep(2)
    out_row = iota((TOK, 64), 0)
    in_row = iota((TOK, 64), 1)
    picks = [
        flag(jnp.logical_and(in_row // 2 == out_row // 8, out_row % 8 == 2 * j + in_row % 2))
        for j in range(4)
    ]
    for x in range(NX):
        result = dot_t(hidden_ref[...], wide(2, range(8), slice(x * 8, (x + 1) * 8)))
        result = result.astype(BF)
        packed = jnp.zeros((TOK, 128), F32)
        for j in range(4):
            packed = packed + dot(picks[j], result[TOK:, j * 128 : (j + 1) * 128])
        out_ref[:, x, :, 0:512] = result[:TOK].reshape(EXPERTS, 8, 512)
        out_ref[:, x, :, 512:640] = packed.astype(BF).reshape(EXPERTS, 8, 128)
    for copy in kept:
        copy.wait()


def ffn(block, both, single):
    sample = jax.ShapeDtypeStruct((EXPERTS, 64, 128), BF)
    return pl.pallas_call(
        ffn_kernel,
        out_shape=(jax.ShapeDtypeStruct((EXPERTS, NX, 8, 640), BF), sample, sample, sample),
        in_specs=[VMEM] + [HBM] * (2 * WAYS),
        out_specs=(VMEM, HBM, HBM, HBM),
        scratch_shapes=[
            pltpu.VMEM((3, 8, EXPERTS, 64, 128), BF),
            pltpu.VMEM((TOK + 64, D), BF),
            pltpu.VMEM((TOK + 64, FF), BF),
            pltpu.SemaphoreType.DMA((3, WAYS)),
            pltpu.SemaphoreType.DMA((3,)),
        ],
        compiler_params=pltpu.CompilerParams(vmem_limit_bytes=52 << 20),
        cost_estimate=pl.CostEstimate(
            flops=6 * 320 * D * FF, bytes_accessed=16 << 20, transcendentals=320 * FF
        ),
        name="ffn",
    )(block, *both, *single)


def mixing_kernel(core_ref, routes_ref, weights_ref, first_ref, last_ref):
    core = core_ref[0]
    expert = iota((TOK, EXPERTS), 1)
    member = jnp.zeros((TOK, EXPERTS), F32)
    weight = jnp.zeros((TOK, EXPERTS), F32)
    for k in range(routes_ref.shape[1]):
        same = routes_ref[:, k : k + 1] == expert
        member = member + jnp.where(same, 1.0, 0.0)
        weight = weight + jnp.where(same, weights_ref[:, k : k + 1], 0.0)
    earlier = flag(iota((TOK, TOK), 1) < iota((TOK, TOK), 0))
    position = dot(earlier, member.astype(BF))
    slot = jnp.where(member > 0.0, position, -1.0).astype(BF)
    spread = flag(iota((EXPERTS, LANES), 1) // (NX * 8) == iota((EXPERTS, LANES), 0))
    slots = dot(slot, spread)
    wide = dot(weight.astype(BF), spread)
    lane = iota((TOK, LANES), 1)
    start = ((lane // 8) % NX * NC + core) * SHARE
    first = slots == (start + lane % 8).astype(F32)
    last = slots == (start + 8 + lane % 2).astype(F32)
    first_ref[...] = jnp.where(first, wide, 0.0).astype(BF)
    last_ref[...] = jnp.where(last, wide, 0.0).astype(BF)


LANES = EXPERTS * NX * 8


def mixing(routes, route_weights, core):
    shape = jax.ShapeDtypeStruct((TOK, LANES), BF)
    return pl.pallas_call(
        mixing_kernel,
        out_shape=(shape, shape),
        in_specs=[SMEM, VMEM, VMEM],
        out_specs=(VMEM, VMEM),
        compiler_params=pltpu.CompilerParams(vmem_limit_bytes=24 << 20),
        cost_estimate=pl.CostEstimate(flops=10**9, bytes_accessed=4 << 20, transcendentals=0),
        name="mixing",
    )(core, routes, route_weights)


def combine_kernel(
    core_ref, back_ref, first_hbm, last_hbm, own_ref, other_ref, first_ref, last_ref, sems
):
    core = core_ref[0]
    copies = [
        pltpu.make_async_copy(source, target, sems.at[i])
        for i, (source, target) in enumerate(
            ((first_hbm, first_ref), (last_hbm, last_ref))
        )
    ]
    for copy in copies:
        copy.start()
    copies[0].wait()
    total = dot(first_ref[...], back_ref[:, 0:512])
    tail = back_ref[:, 512:640]
    lane = iota((TOK, LANES), 1)
    copies[1].wait()
    last = last_ref[...]
    pieces = []
    for j in range(4):
        mine = lane % 8 // 2 == j
        pieces.append(dot(jnp.where(mine, last, jnp.zeros_like(last)), tail))
    total = total + jnp.concatenate(pieces, axis=1)
    left, right = total[:, :256], total[:, 256:]
    own_ref[...] = jnp.where(core == 0, left, right)
    other_ref[...] = jnp.where(core == 0, right, left).astype(BF)


def combine(back, mix, core):
    return pl.pallas_call(
        combine_kernel,
        out_shape=(
            jax.ShapeDtypeStruct((TOK, 256), F32),
            jax.ShapeDtypeStruct((TOK, 256), BF),
        ),
        in_specs=[SMEM, VMEM, HBM, HBM],
        out_specs=(VMEM, VMEM),
        scratch_shapes=[
            pltpu.VMEM((TOK, LANES), BF),
            pltpu.VMEM((TOK, LANES), BF),
            pltpu.SemaphoreType.DMA((2,)),
        ],
        compiler_params=pltpu.CompilerParams(vmem_limit_bytes=52 << 20),
        cost_estimate=pl.CostEstimate(flops=10**9, bytes_accessed=4 << 20, transcendentals=0),
        name="combine",
    )(core, back, *mix)


def shared_kernel(at_ref, normed_ref, *refs):
    block_refs, mine_ref, other_ref = refs[:NY], refs[NY], refs[NY + 1]
    common_refs = refs[NY + 2 :]
    z, y, core = at_ref[0], at_ref[1], at_ref[2]
    for dy in range(NY):
        for dz in range(NZ):
            row = ((z + dz) % NZ * NY + (y + dy) % NY) * 64
            part = pl.ds(pl.multiple_of(row, 64), 64)
            for n in range(3):
                common_refs[n][part, :] = block_refs[dy][dz, :, n * 128 : (n + 1) * 128]
    both = jnp.concatenate([common_refs[0][...], common_refs[1][...]], axis=1)
    act = dot(normed_ref[...], both)
    gate, up = act[:, 0:128], act[:, 128:256]
    hidden = (gate / (1.0 + jnp.exp(-gate)) * up).astype(BF)
    for x in range(NX):
        term = dot_t(hidden, common_refs[2][x * 512 : (x + 1) * 512, :])
        left, right = term[:, :256], term[:, 256:]
        mine_ref[x] = jnp.where(core == 0, left, right).astype(BF)
        other_ref[x] = jnp.where(core == 0, right, left).astype(BF)


def shared_expert(normed, blocks, at):
    shape = jax.ShapeDtypeStruct((D, 128), BF)
    terms = jax.ShapeDtypeStruct((NX, TOK, 256), BF)
    return pl.pallas_call(
        shared_kernel,
        out_shape=(terms, terms, shape, shape, shape),
        in_specs=[SMEM] + [VMEM] * (1 + NY),
        out_specs=(VMEM,) * 5,
        compiler_params=pltpu.CompilerParams(vmem_limit_bytes=24 << 20),
        cost_estimate=pl.CostEstimate(
            flops=6 * TOK * D * 128, bytes_accessed=6 << 20, transcendentals=TOK * 128
        ),
        name="shared_expert",
    )(at, normed, *blocks)


def pair_kernel(at_ref, mine_ref, swapped_ref, *out_refs):
    for dx in range(NX):
        x = (at_ref[0] + dx) % NX
        total = mine_ref[x].astype(F32) + swapped_ref[x].astype(F32)
        out_refs[dx][...] = total.astype(BF)


def pair_sum(mine, swapped, at):
    shape = jax.ShapeDtypeStruct((TOK, 256), BF)
    return pl.pallas_call(
        pair_kernel,
        out_shape=(shape,) * NX,
        in_specs=[SMEM, VMEM, VMEM],
        out_specs=(VMEM,) * NX,
        compiler_params=pltpu.CompilerParams(vmem_limit_bytes=8 << 20),
        cost_estimate=pl.CostEstimate(flops=10**6, bytes_accessed=2 << 20, transcendentals=0),
        name="pair_sum",
    )(at, mine, swapped)


def exchange(array, axes):
    return lax.all_to_all(array, axes, split_axis=0, concat_axis=0, tiled=True)


def after(*arrays):
    return lax.optimization_barrier(arrays)


def to_neighbours(rows):
    return shift(rows, "x", NX, 1), shift(rows, "x", NX, -1)


def to_opposite(near):
    return shift(near[0][:HALF], "x", NX, 1), shift(near[1][HALF:], "x", NX, -1)


def layer(
    tokens,
    routes,
    route_weights,
    norm_gain,
    expert_gate,
    expert_up,
    expert_down,
    shared_gate,
    shared_up,
    shared_down,
):
    z, y, x, c = (lax.axis_index(a).astype(jnp.int32) for a in FS + TP)
    at = (x * NC + c).reshape(1)
    core = c.reshape(1)

    shared = jnp.concatenate(
        [
            (shared_gate * norm_gain[:, None]).astype(BF),
            (shared_up * norm_gain[:, None]).astype(BF),
            shared_down.astype(BF),
        ],
        axis=1,
    )
    column = [shared] + [shift(shared, "z", NZ, -k) for k in range(1, NZ)]
    column = jnp.stack(column)
    blocks = [column] + [shift(column, "y", NY, -k) for k in range(1, NY)]

    both_in = round_both(norm_gain, expert_gate, expert_up)
    both_in, expert_down = after(both_in, expert_down)
    down_in = expert_down.astype(BF)
    packed, normed = dispatch(tokens, routes.T, at)

    both_rows = exchange(both_in, FS)

    down_in, both_rows = after(down_in, both_rows)
    down_rows = exchange(down_in, FS)
    both_near = to_neighbours(both_rows)

    packed, down_rows = after(packed, down_rows)
    block = exchange(packed.reshape(EXPERTS, 8, D + 512), FS).reshape(TOK, D + 512)
    both_far = to_opposite(both_near)
    down_near = to_neighbours(down_rows)
    down_far = to_opposite(down_near)
    both_all = [both_rows, *both_near, *both_far]
    down_all = [down_rows, *down_near, *down_far]
    both_all += [shift(piece, "c", NC, 1) for piece in both_all]
    down_all += [shift(piece, "c", NC, 1) for piece in down_all]

    mine, other, common_gate, common_up, common_down = shared_expert(
        normed, blocks, jnp.stack([z, y, c])
    )
    swapped = shift(other, "c", NC, 1)
    sums = pair_sum(mine, swapped, x.reshape(1))
    sums = [sums[0]] + [shift(sums[k], "x", NX, k) for k in range(1, NX)]

    results, sample_gate, sample_up, sample_down = ffn(block, both_all, down_all)
    mix = mixing(routes, route_weights, core)
    back = exchange(results.reshape(EXPERTS * NX, 8, 640), ("z", "y", "x"))
    own, other = combine(back.reshape(EXPERTS * NX * 8, 640), mix, core)
    other = shift(other, "c", NC, 1)
    shared_sum = sum(part.astype(F32) for part in sums)
    layer_output = (own + other.astype(F32) + shared_sum).astype(BF)
    return (
        layer_output,
        sample_gate.reshape(1, D, 128),
        sample_up.reshape(1, D, 128),
        sample_down.reshape(1, D, 128),
        common_gate,
        common_up,
        common_down,
    )


def solution(mesh):
    mesh = Mesh(mesh.devices.reshape(NZ, NY, NX, NC), FS + TP)
    return jax.shard_map(
        layer,
        mesh=mesh,
        in_specs=(
            P(FS, None),
            P(FS, None),
            P(FS, None),
            P(FS),
            P(None, FS, TP),
            P(None, FS, TP),
            P(None, FS, TP),
            P(FS, TP),
            P(FS, TP),
            P(FS, TP),
        ),
        out_specs=(
            P(FS, TP),
            P(FS, None, TP),
            P(FS, None, TP),
            P(FS, None, TP),
            P(None, TP),
            P(None, TP),
            P(None, TP),
        ),
        check_vma=False,
    )
```
